32 devices in a mesh: grp: 2 (over y), ep: 4 (over z), tp: 4 (over x, core).
Axes of the slice: x: 2, y: 2, z: 4, core: 2. Of those that a mesh axis runs over, the one named last changes fastest.
Arguments:
- scan_branch_source: bfloat16 [1024, 1344], P(('grp', 'ep'), 'tp'), parts along dimension 0, may hold values from -8 to 8
- valve_branch_source: bfloat16 [1024, 1344], P(('grp', 'ep'), 'tp'), parts along dimension 0, may hold values from -6 to 6
- stencil_factors: bfloat16 [4, 1344], P(None, 'tp'), may hold values from -3 to 3
- carry_valve_matrix: bfloat16 [8, 168, 168], P('tp'), may hold values from -0.5 to 0.5
- entry_valve_matrix: bfloat16 [8, 168, 168], P('tp'), may hold values from -0.5 to 0.5
- lane_fade_param: float32 [1344], P('tp'), may hold values from 0 to 16
- jump_log_fade: float32 [1024], P(('grp', 'ep')), parts along dimension 0, may hold values from -0.6 to 0, as said below
- specialist_entries: bfloat16 [2048, 2048], P(('grp', 'ep')), parts along dimension 0, may hold values from -6 to 6
- specialist_rms_scale: float32 [2048], replicated, may hold values from 0.1 to 1.9
- assigned_specialists: int32 [2048, 2], P(('grp', 'ep')), parts along dimension 0, may hold values from 0 to 3, all different within a row; in each aligned block of 256 rows (0 to 255, 256 to 511, ...) at most 192 rows name the same one
- picked_route_scores: float32 [2048, 2], P(('grp', 'ep')), parts along dimension 0, may hold values from -6 to 6
- expand_matrix: bfloat16 [4, 2048, 3584], P('ep', None, 'tp'), may hold values from -0.125 to 0.125
- contract_matrix: bfloat16 [4, 3584, 2048], P('ep', None, 'tp'), may hold values from -0.09375 to 0.09375
Outputs:
- valved_scan_target: bfloat16 [1024, 1344], P(('grp', 'ep'), 'tp'), parts along dimension 0
- moe_out: bfloat16 [2048, 2048], P(('grp', 'ep'), 'tp'), parts along dimension 0
The draws below stay inside these ranges and needn't reach their ends.
There are 2 independent parts, one for each index of `grp`. The reference program is written for one: setup_inputs(seed, part) draws one part's arguments, and reference() takes and returns one part's arrays. A program takes and returns all parts, laid end to end along the dimension named above; an argument that names none is the same for every part. Nothing has to cross between parts.
Inputs may be any that keep to these rules, and one draw needn't show every extreme that they name: `assigned_specialists`: each row names 2 different experts. Among the tokens of one index of ep (aligned blocks of 256 rows) no expert is named more than 192 times, and in some block some expert is named exactly 192 times. `jump_log_fade`: zero at all but a few positions.
All inputs are finite; a program needn't handle non-finite values.
Results may differ from the reference program's by a relative error of at most 0.0065.
Values may be sent and summed in bfloat16 or wider, within the bound.
A program may use at most 128 MiB of HBM per device.

```python
import math
from functools import partial
import jax
import jax.numpy as jnp
import numpy as np
from jax import lax

D = 2048
FF = 3584
BW = 168
BLOCKS = 8
CONV = 4
TOPK = 2
MX_DEV = 128
MT_DEV = 256
CH = 1344
EXPERTS = 4
SEQUENCE_POINTS = 512
MTOK = 1024
CAP = 192
N_EP = 4


def draw_scan_branch_source(key, part):
    scale_key, base_key = jax.random.split(jax.random.fold_in(key, 11))
    block_count = SEQUENCE_POINTS // MX_DEV
    scales = jnp.exp(jax.random.uniform(scale_key, (block_count,), jnp.float32, jnp.log(0.5), jnp.log(2.0)))
    row_scale = scales[jnp.arange(SEQUENCE_POINTS) // MX_DEV]
    base_draw = jnp.clip(jax.random.normal(base_key, (SEQUENCE_POINTS, CH), jnp.float32), -4.0, 4.0)
    return (base_draw * row_scale[:, None]).astype(jnp.bfloat16)


def draw_lane_fade_param(key, part):
    pick_key, fast_key, slow_key = jax.random.split(jax.random.fold_in(key, 23), 3)
    fast_share = 0.5
    fast_pick = jax.random.bernoulli(pick_key, fast_share, (CH,))
    fast_rate = jnp.exp(jax.random.uniform(fast_key, (CH,), jnp.float32, jnp.log(1.0 / MX_DEV), jnp.log(3.0 / MX_DEV)))
    slow_rate = jnp.exp(jax.random.uniform(slow_key, (CH,), jnp.float32, jnp.log(0.01 / SEQUENCE_POINTS), jnp.log(0.1 / SEQUENCE_POINTS)))
    decay_rate = jnp.where(fast_pick, fast_rate, slow_rate)
    return (-jnp.log(jnp.expm1(decay_rate))).astype(jnp.float32)


def draw_jump_log_fade(key, part):
    location_random_key, height_random_key = jax.random.split(jax.random.fold_in(key, 37))
    spike_locations = jax.random.randint(location_random_key, (3,), 0, SEQUENCE_POINTS)
    spike_height = jax.random.uniform(height_random_key, (3,), jnp.float32, jnp.log(0.55), jnp.log(0.8))
    return jnp.zeros((SEQUENCE_POINTS,), jnp.float32).at[spike_locations].set(spike_height)


def levels(own_key, extent, cuts, least, top_value):
    loudness, own = 1.0, jax.random.fold_in(own_key, 6)
    for dim, parts in cuts:
        steps = jnp.exp(jax.random.uniform(jax.random.fold_in(own, dim), (parts,), jnp.float32, least / len(cuts), top_value / len(cuts)))
        loudness = loudness * jnp.repeat(steps, extent[dim] // parts).reshape([-1 if axis == dim else 1 for axis in range(len(extent))])
    return loudness


def shared_out(own_key, own, number, rows, count, top, reach, skew):
    sequence = jax.random.permutation(own_key, count)
    crowded, common = portions_of(count, rows * top, reach, skew, True), portions_of(count, rows * top, reach, skew, False)
    places = jnp.arange(count)

    def named(tallies, offset_by):
        used = int((tallies > 0).sum())
        fixed = max(1, used // 4)
        shifted = fixed + (places - fixed + offset_by * (used - fixed)) % max(1, count - fixed)
        return jnp.zeros((count,), jnp.int32).at[sequence[jnp.where(places < fixed, places, shifted)]].set(jnp.asarray(tallies, jnp.int32))

    tallies = jnp.where(number % 4 == 0, named(crowded, number // 4), named(common, number - number // 4 - 1))
    mixed = jax.random.permutation(jax.random.fold_in(own, 3), count)
    donor, receiver = mixed[0:count // 2 * 2:2], mixed[1:count // 2 * 2:2]
    margin = jnp.minimum(tallies[donor] - 1, reach - tallies[receiver]) // 2
    margin = jnp.where((donor == sequence[0]) | (receiver == sequence[0]) | (tallies[receiver] == 0), 0, jnp.maximum(margin, 0))
    shifted = jax.random.randint(jax.random.fold_in(own, 4), (count // 2,), 0, 1 << 20) % (margin + 1)
    tallies = tallies.at[donor].add(-shifted).at[receiver].add(shifted)
    members = jnp.searchsorted(jnp.cumsum(tallies), jnp.arange(rows * top), side="right").astype(jnp.int32)
    listing = members.reshape(top, rows).T
    listing = listing[jax.random.permutation(jax.random.fold_in(own, 1), rows)]
    offset_by = jax.random.randint(jax.random.fold_in(own, 2), (rows, 1), 0, top)
    return jnp.take_along_axis(listing, (jnp.arange(top)[None, :] + offset_by) % top, axis=1)


def portions_of(count, total, bound, lean, full):
    loads = [(1 << 20) // math.isqrt(grade ** lean) + 1 for grade in range(1, count + 1)]
    largest = bound if full else min(bound, max(-(-total // count), total * loads[0] // sum(loads)))
    least = 1 if total - largest >= count - 1 else 0
    counts, rest = [largest] + [least] * (count - 1), total - largest - least * (count - 1)
    while rest > 0:
        movable = [i for i in range(1, count) if counts[i] < largest] or [i for i in range(1, count) if counts[i] < bound]
        whole, budget = sum([loads[i] for i in movable]), rest
        for i in movable:
            addition = min(bound - counts[i], max(1, budget * loads[i] // whole), rest)
            counts[i] = counts[i] + addition
            rest = rest - addition
    return np.array(counts)


def scatter_about(key, dims, deviation, bound, pieces=(), kind=jnp.bfloat16):
    result = jax.random.normal(key, dims, jnp.float32) * deviation
    if len(pieces) > 0:
        result = levels(key, dims, pieces, -0.22, 0.18) * result
    return jnp.clip(result, min=-bound, max=bound).astype(kind)


def setup_inputs(seed: int = 0, part: int = 0) -> dict:
    key_of = jax.random.split(jax.random.key(seed), 14)
    own_keys = jax.random.split(jax.random.fold_in(key_of[13], part), 14)
    scan_branch_source = draw_scan_branch_source(jax.random.fold_in(jax.random.fold_in(key_of[13], part), 71), part)
    valve_branch_source = scatter_about(own_keys[1], (SEQUENCE_POINTS, CH), 1.0, 6.0, ((0, 4), (1, 4)))
    stencil_factors = scatter_about(key_of[2], (CONV, CH), CONV ** -0.5, 3.0, ((1, 4),))
    carry_valve_matrix = scatter_about(key_of[3], (BLOCKS, BW, BW), BW ** -0.5, 0.5, ((0, 4),))
    entry_valve_matrix = scatter_about(key_of[4], (BLOCKS, BW, BW), BW ** -0.5, 0.5, ((0, 4),))
    lane_fade_param = draw_lane_fade_param(jax.random.fold_in(key_of[13], 71), part)
    jump_log_fade = draw_jump_log_fade(jax.random.fold_in(jax.random.fold_in(key_of[13], part), 71), part)
    specialist_entries = scatter_about(own_keys[7], (MTOK, D), 1.0, 6.0, ((0, 4),))
    specialist_rms_scale = jnp.clip(1.0 + 0.18 * jax.random.normal(key_of[8], (D,), jnp.float32), 0.1, 1.9)
    assigned_specialists_keys = jax.random.split(jax.random.fold_in(own_keys[9], 1), MTOK // MT_DEV)
    assigned_specialists_turns = jax.random.permutation(jax.random.fold_in(own_keys[9], 3), MTOK // MT_DEV)
    assigned_specialists = jax.vmap(lambda own, number: shared_out(jax.random.fold_in(own_keys[9], 2), own, number, MT_DEV, EXPERTS, TOPK, CAP, 1))(assigned_specialists_keys, assigned_specialists_turns).reshape((MTOK, TOPK))
    picked_route_scores = scatter_about(own_keys[10], (MTOK, TOPK), 1.5, 6.0, ((0, 4),), jnp.float32)
    expand_matrix = scatter_about(key_of[11], (EXPERTS, D, FF), D ** -0.5, 0.125, ((0, 4), (2, 4)))
    contract_matrix = scatter_about(key_of[12], (EXPERTS, FF, D), FF ** -0.5, 0.09375, ((0, 4), (2, 4)))
    return dict(scan_branch_source=scan_branch_source, valve_branch_source=valve_branch_source, stencil_factors=stencil_factors, carry_valve_matrix=carry_valve_matrix, entry_valve_matrix=entry_valve_matrix, lane_fade_param=lane_fade_param, jump_log_fade=jump_log_fade, specialist_entries=specialist_entries, specialist_rms_scale=specialist_rms_scale, assigned_specialists=assigned_specialists, picked_route_scores=picked_route_scores, expand_matrix=expand_matrix, contract_matrix=contract_matrix)


def chain_link(earlier, later):
    early_decay, early_state = earlier
    late_decay, late_state = later
    return (early_decay * late_decay, late_decay * early_state + late_state)

def slot_table(assigned_specialists, experts, capacity):
    flat_routes = assigned_specialists.reshape(-1)
    top_count = assigned_specialists.shape[1]
    matches = (flat_routes[:, None] == jnp.arange(experts, dtype=jnp.int32)[None, :]).astype(jnp.int32)
    before = jnp.cumsum(matches, axis=0) - matches
    slot_rank = lax.optimization_barrier(jnp.sum(before * matches, axis=1))
    slot_index = (flat_routes * capacity + slot_rank).astype(jnp.int32)
    owner_row = (jnp.arange(flat_routes.shape[0], dtype=jnp.int32) // top_count).astype(jnp.int32)
    source = jnp.zeros((experts * capacity,), jnp.int32).at[slot_index].set(owner_row)
    filled = jnp.zeros((experts * capacity,), jnp.float32).at[slot_index].set(1.0)
    return (slot_index, source, filled)

def temporal_block_part(scan_branch_source, valve_branch_source, stencil_factors, carry_valve_matrix, entry_valve_matrix, lane_fade_param, jump_log_fade):
    length = scan_branch_source.shape[0]
    channels = scan_branch_source.shape[1]
    padded = jnp.pad(scan_branch_source.astype(jnp.float32), ((CONV - 1, 0), (0, 0)))
    tap_values = stencil_factors.astype(jnp.float32)
    conv_out = jnp.zeros((length, channels), jnp.float32)
    for offset in range(CONV):
        conv_out = conv_out + padded[offset:offset + length] * tap_values[offset]
    conv_half = lax.optimization_barrier(conv_out.astype(jnp.bfloat16))
    conv_blocks = conv_half.astype(jnp.float32).reshape(length, BLOCKS, BW)
    carry_valve = jax.nn.sigmoid(jnp.einsum('tnc,ncd->tnd', conv_blocks, carry_valve_matrix.astype(jnp.float32), precision=lax.Precision.HIGHEST).reshape(length, channels))
    input_gate = jax.nn.sigmoid(jnp.einsum('tnc,ncd->tnd', conv_blocks, entry_valve_matrix.astype(jnp.float32), precision=lax.Precision.HIGHEST).reshape(length, channels))
    fade_log_rate = -8.0 * carry_valve * jax.nn.softplus(-lane_fade_param)[None, :] + jump_log_fade[:, None]
    drive_term = jnp.sqrt(-jnp.expm1(2.0 * fade_log_rate)) * input_gate * conv_out
    cumulative, hidden_state = lax.associative_scan(chain_link, (jnp.exp(fade_log_rate), drive_term), axis=0)
    return (hidden_state * jax.nn.gelu(valve_branch_source.astype(jnp.float32))).astype(jnp.bfloat16)

def expert_part(specialist_entries, specialist_rms_scale, assigned_specialists, picked_route_scores, expand_matrix, contract_matrix):
    tok_rows = specialist_entries.astype(jnp.float32)
    row_mean = lax.optimization_barrier(jnp.mean(tok_rows, axis=1, keepdims=True))
    centered = tok_rows - row_mean
    row_var = lax.optimization_barrier(jnp.mean(centered * centered, axis=1, keepdims=True))
    normed = (centered * lax.rsqrt(row_var + 1e-05) * specialist_rms_scale[None, :]).astype(jnp.bfloat16)
    blocks = assigned_specialists.reshape(N_EP, MT_DEV, TOPK)
    slots, sources, filled = jax.vmap(partial(slot_table, experts=EXPERTS, capacity=CAP))(blocks)
    offsets = (jnp.arange(N_EP, dtype=jnp.int32) * MT_DEV)[:, None]
    global_source = (sources + offsets).reshape(N_EP, EXPERTS, CAP).transpose(1, 0, 2)
    global_filled = filled.reshape(N_EP, EXPERTS, CAP).transpose(1, 0, 2)

    def one_expert(inputs):
        source, mask_rows, up_part, down_part = inputs
        picked = normed[source.reshape(-1)] * mask_rows.reshape(-1, 1).astype(jnp.bfloat16)
        hidden = jax.nn.silu(jnp.dot(picked, up_part, preferred_element_type=jnp.float32)).astype(jnp.bfloat16)
        return jnp.dot(hidden, down_part, preferred_element_type=jnp.float32).astype(jnp.bfloat16)
    results = lax.map(one_expert, (global_source, global_filled, expand_matrix, contract_matrix))
    results = results.reshape(EXPERTS, N_EP, CAP, D)
    slot_index = slots.reshape(N_EP, MT_DEV * TOPK)
    expert_index = slot_index // CAP
    rank_index = slot_index % CAP
    block_index = jnp.broadcast_to(jnp.arange(N_EP, dtype=jnp.int32)[:, None], slot_index.shape)
    picked = results[expert_index, block_index, rank_index].reshape(MTOK, TOPK, D).astype(jnp.float32)
    first_weight = jax.nn.sigmoid(picked_route_scores[:, 0] - picked_route_scores[:, 1])
    weights = jnp.stack([first_weight, 1.0 - first_weight], axis=1)
    return lax.optimization_barrier(jnp.sum(weights[:, :, None] * picked, axis=1)).astype(jnp.bfloat16)

def reference(scan_branch_source, valve_branch_source, stencil_factors, carry_valve_matrix, entry_valve_matrix, lane_fade_param, jump_log_fade, specialist_entries, specialist_rms_scale, assigned_specialists, picked_route_scores, expand_matrix, contract_matrix):
    valved_scan_target = temporal_block_part(scan_branch_source, valve_branch_source, stencil_factors, carry_valve_matrix, entry_valve_matrix, lane_fade_param, jump_log_fade)
    moe_out = expert_part(specialist_entries, specialist_rms_scale, assigned_specialists, picked_route_scores, expand_matrix, contract_matrix)
    return (valved_scan_target, moe_out)
```

```python
import functools

import jax
import jax.numpy as jnp
from jax import lax
from jax.experimental import pallas as pl
from jax.experimental.pallas import tpu as pltpu
from jax.sharding import PartitionSpec as P

CONV = 4


def passed_along(block, axis, distance):
    devices = range(lax.axis_size(axis))
    route = [(i - distance, i) for i in devices if i - distance in devices]
    return lax.ppermute(block, axis, route)


def carried_in(part, axis, combine, identity):
    place = lax.axis_index(axis)
    gathered = jax.tree.map(lambda a: lax.all_gather(a, axis), part)
    state = jax.tree.map(lambda a, e: jnp.zeros_like(a) + jnp.asarray(e, a.dtype), part, identity)

    def one(step, state):
        return combine(
            state, jax.tree.map(lambda a: lax.dynamic_index_in_dim(a, step, 0, False), gathered)
        )

    return lax.fori_loop(0, place, one, state)


def chain_link(earlier, later):
    early_decay, early_state = earlier
    late_decay, late_state = later
    return (early_decay * late_decay, late_decay * early_state + late_state)


def slot_table(assigned_specialists, experts, capacity):
    flat_routes = assigned_specialists.reshape(-1)
    top_count = assigned_specialists.shape[1]
    matches = (flat_routes[:, None] == jnp.arange(experts, dtype=jnp.int32)[None, :]).astype(
        jnp.int32
    )
    before = jnp.cumsum(matches, axis=0) - matches
    slot_rank = jnp.sum(before * matches, axis=1)
    slot_index = flat_routes * capacity + slot_rank
    owner_row = jnp.arange(flat_routes.shape[0], dtype=jnp.int32) // top_count
    source = jnp.zeros((experts * capacity,), jnp.int32).at[slot_index].set(owner_row)
    filled = jnp.zeros((experts * capacity,), jnp.float32).at[slot_index].set(1.0)
    return (slot_index, source, filled)


def temporal_block_part(
    scan_branch_source,
    valve_branch_source,
    stencil_factors,
    carry_valve_matrix,
    entry_valve_matrix,
    lane_fade_param,
    jump_log_fade,
):
    length = scan_branch_source.shape[0]
    channels = scan_branch_source.shape[1]
    previous = passed_along(scan_branch_source[length - (CONV - 1) :], "ep", 1)
    padded = jnp.concatenate([previous, scan_branch_source], axis=0).astype(jnp.float32)
    tap_values = stencil_factors.astype(jnp.float32)
    conv_out = jnp.zeros((length, channels), jnp.float32)
    for offset in range(CONV):
        conv_out = conv_out + padded[offset : offset + length] * tap_values[offset]
    blocks_here = carry_valve_matrix.shape[0]
    conv_blocks = conv_out.astype(jnp.bfloat16).reshape(
        length, blocks_here, carry_valve_matrix.shape[1]
    )
    carry_valve = jax.nn.sigmoid(
        jnp.einsum(
            "tnc,ncd->tnd", conv_blocks, carry_valve_matrix, preferred_element_type=jnp.float32
        ).reshape(length, channels)
    )
    input_gate = jax.nn.sigmoid(
        jnp.einsum(
            "tnc,ncd->tnd", conv_blocks, entry_valve_matrix, preferred_element_type=jnp.float32
        ).reshape(length, channels)
    )
    fade_log_rate = (
        -8.0 * carry_valve * jax.nn.softplus(-lane_fade_param)[None, :] + jump_log_fade[:, None]
    )
    drive_term = jnp.sqrt(-jnp.expm1(2.0 * fade_log_rate)) * input_gate * conv_out
    cumulative, local_state = lax.associative_scan(
        chain_link, (jnp.exp(fade_log_rate), drive_term), axis=0
    )
    identity = (jnp.ones((channels,), jnp.float32), jnp.zeros((channels,), jnp.float32))
    entering = carried_in((cumulative[-1], local_state[-1]), "ep", chain_link, identity)
    hidden_state = local_state + cumulative * entering[1][None, :]
    return (hidden_state * jax.nn.gelu(valve_branch_source.astype(jnp.float32))).astype(
        jnp.bfloat16
    )


def expert_part(
    specialist_entries,
    specialist_rms_scale,
    assigned_specialists,
    picked_route_scores,
    expand_matrix,
    contract_matrix,
):
    ep_size = lax.axis_size("ep")
    tp_size = lax.axis_size("tp")
    exp_dev = expand_matrix.shape[0]
    experts = exp_dev * ep_size
    tokens = specialist_entries.shape[0]
    features = specialist_entries.shape[1]
    top_count = assigned_specialists.shape[1]
    capacity = tp_size * (
        (3 * tokens * top_count + 2 * experts * tp_size - 1) // (2 * experts * tp_size)
    )
    tok_rows = specialist_entries.astype(jnp.float32)
    row_mean = jnp.mean(tok_rows, axis=1, keepdims=True)
    centered = tok_rows - row_mean
    row_var = jnp.mean(centered * centered, axis=1, keepdims=True)
    normed = (centered * lax.rsqrt(row_var + 1e-05) * specialist_rms_scale[None, :]).astype(
        jnp.bfloat16
    )
    slot_index, source, filled = slot_table(assigned_specialists, experts, capacity)
    source_grid = source.reshape(experts, capacity)
    filled_grid = filled.reshape(experts, capacity)
    slice_size = capacity // tp_size
    first_slot = lax.axis_index("tp") * slice_size
    source_grid = lax.dynamic_slice_in_dim(source_grid, first_slot, slice_size, 1)
    filled_grid = lax.dynamic_slice_in_dim(filled_grid, first_slot, slice_size, 1)
    outgoing = normed[source_grid] * filled_grid[:, :, None].astype(jnp.bfloat16)
    outgoing = outgoing.reshape(ep_size, exp_dev, source_grid.shape[1], features)
    arrived = lax.all_to_all(outgoing, "ep", split_axis=0, concat_axis=0, tiled=True)
    arrived = lax.all_gather(arrived, "tp", axis=2, tiled=True)
    hidden = jax.nn.silu(
        jnp.einsum("secd,edf->secf", arrived, expand_matrix, preferred_element_type=jnp.float32)
    ).astype(jnp.bfloat16)
    column_count = contract_matrix.shape[2]
    expert_out = jnp.einsum(
        "secf,efd->secd",
        lax.all_gather(hidden, "tp", axis=3, tiled=True),
        contract_matrix,
        preferred_element_type=jnp.float32,
    ).astype(jnp.bfloat16)
    returned = lax.all_to_all(expert_out, "ep", split_axis=0, concat_axis=0, tiled=True)
    returned = returned.reshape(experts * capacity, column_count)
    picked = returned[slot_index].reshape(tokens, top_count, column_count).astype(jnp.float32)
    first_weight = jax.nn.sigmoid(picked_route_scores[:, 0] - picked_route_scores[:, 1])
    weights = jnp.stack([first_weight, 1.0 - first_weight], axis=1)
    return jnp.sum(weights[:, :, None] * picked, axis=1).astype(jnp.bfloat16)


MESH = pl.DeviceIdType.MESH
HALO = 16


def remote(src, dst, sems, index, **device):
    return pltpu.make_async_remote_copy(
        src_ref=src,
        dst_ref=dst,
        send_sem=sems.at[0, index],
        recv_sem=sems.at[1, index],
        device_id=device,
        device_id_type=MESH,
    )


def as_column(row):
    n = row.shape[1]
    same = lax.broadcasted_iota(jnp.int32, (n, n), 0) == lax.broadcasted_iota(jnp.int32, (n, n), 1)
    return jnp.sum(jnp.where(same, row, 0.0), axis=1, keepdims=True)


def one_minus_exp(x):
    near = jnp.maximum(x, -0.35)
    series = 1.0 + near * (1.0 / 8.0)
    for divisor in (7.0, 6.0, 5.0, 4.0, 3.0, 2.0):
        series = 1.0 + near * (1.0 / divisor) * series
    return jnp.where(x > -0.35, -near * series, 1.0 - jnp.exp(x))


OWN, NEAR, INNER, OUTER = 0, 1, 2, 3
PARTS = {OWN: 3, NEAR: 3, INNER: 3, OUTER: 3}
ORDER = (
    "D31", "D21", "D32", "P01", "D13", "T31", "P02", "F31", "T21", "D22", "D11", "M31",
    "T22", "T13", "F13", "F21", "D33", "T11", "D23", "F11", "T32", "D12", "M21", "F22",
    "T33", "F32", "M32", "G31", "M22", "T23", "S31", "A", "T12", "F12", "F33", "M33",
    "M11", "G32", "G21", "G01", "M12", "F23", "S32", "M23", "M13", "S21", "G33", "S33",
    "P03", "G11", "G22", "S11", "S22", "B", "G12", "S12", "G02", "G23", "S23", "G13",
    "S13", "G03", "S01", "S03", "S02", "C0", "C2", "C3", "C1",
)


def fused_kernel(
    n,
    capacity,
    scan_ref,
    valve_ref,
    taps_ref,
    carry_w_ref,
    entry_w_ref,
    lane_ref,
    jump_ref,
    tok_ref,
    gain_ref,
    route_ref,
    score_ref,
    up_hbm,
    down_hbm,
    scan_out,
    moe_out,
    up,
    down,
    normed,
    rank_rows,
    near_rows,
    cross_rows,
    toks,
    hid,
    res,
    back,
    acc,
    chosen,
    share,
    total,
    halo,
    padded,
    conv_buf,
    decay_buf,
    state_buf,
    carry_out,
    carry_in,
    halo_out,
    load_sems,
    zt,
    tx,
    tm,
    tf,
    hx,
    hm,
    hf,
    rz,
    halo_sems,
    carry_sems,
):
    e = lax.axis_index("ep")
    t = lax.axis_index("tp")
    mate = t + 1 - 2 * (t % 2)
    across = (t + 2) % 4
    far = (mate + 2) % 4
    upper = e // 2
    peer = {NEAR: e + 1 - 2 * (e % 2), INNER: 2 - upper, OUTER: 3 - 3 * upper}
    cross_slot = OUTER - (e + upper) % 2
    slot_there = {NEAR: NEAR, INNER: cross_slot, OUTER: cross_slot}
    tokens, features = tok_ref.shape
    part = features // 4
    width = up.shape[1]
    out_width = down.shape[1]

    def f_cols(i):
        return pl.ds(pl.multiple_of(i * part, part), part)

    def half_cols(i):
        return pl.ds(pl.multiple_of((i % 2) * 2 * part, 2 * part), 2 * part)

    def h_cols(i):
        return pl.ds(pl.multiple_of(i * width, 128), width)

    def piece(slot, c):
        size = capacity // PARTS[slot]
        return pl.ds(c * size, size)

    barrier = pltpu.get_barrier_semaphore()
    for j in range(1, n):
        pl.semaphore_signal(barrier, inc=1, device_id={"ep": (e + j) % n}, device_id_type=MESH)
    for other in (mate, across):
        pl.semaphore_signal(barrier, inc=1, device_id={"tp": other}, device_id_type=MESH)
    load_up = pltpu.make_async_copy(up_hbm.at[0], up, load_sems.at[0])
    load_down = pltpu.make_async_copy(down_hbm.at[0], down, load_sems.at[1])
    load_up.start()
    load_down.start()
    channels, length = scan_ref.shape

    with jax.named_scope("halo_prep"):
        turned = scan_ref[...].astype(jnp.float32).T
        padded[HALO:, :] = turned
        halo_out[...] = turned[length - HALO :, :].astype(jnp.bfloat16)

    rows_step = 64

    def norm_rows(i, _):
        rows = pl.ds(pl.multiple_of(i * rows_step, rows_step), rows_step)
        x = tok_ref[rows, :].astype(jnp.float32)
        centered = x - jnp.sum(x, axis=1, keepdims=True) * (1.0 / features)
        var = jnp.sum(centered * centered, axis=1, keepdims=True) * (1.0 / features)
        normed[rows, :] = (centered * lax.rsqrt(var + 1e-05) * gain_ref[...]).astype(jnp.bfloat16)
        return 0

    with jax.named_scope("norm"):
        lax.fori_loop(0, tokens // rows_step, norm_rows, 0)

    with jax.named_scope("rank"):
        routes = route_ref[...].astype(jnp.float32)
        first, second = routes[0:1, :], routes[1:2, :]
        erow = lax.broadcasted_iota(jnp.int32, (rank_rows.shape[0], tokens), 0).astype(jnp.float32)
        hit = (erow == first) | (erow == second)
        ti = lax.broadcasted_iota(jnp.int32, (tokens, tokens), 0)
        tj = lax.broadcasted_iota(jnp.int32, (tokens, tokens), 1)
        rank = jnp.dot(
            hit.astype(jnp.float32).astype(jnp.bfloat16),
            (ti < tj).astype(jnp.float32).astype(jnp.bfloat16),
            preferred_element_type=jnp.float32,
        )
        rank_rows[...] = jnp.where(hit, rank, -1.0)

    def picker(expert, start, size):
        slots = start + lax.broadcasted_iota(jnp.int32, (size, tokens), 0)
        hits = slots.astype(jnp.float32) == rank_rows[pl.ds(expert, 1), :]
        return hits.astype(jnp.float32).astype(jnp.bfloat16)

    with jax.named_scope("barrier"):
        pl.semaphore_wait(barrier, n + 1)

    send_halo = remote(halo_out, halo, halo_sems, 0, ep=(e + 1) % n)
    send_halo.start()
    sent = [send_halo]
    waited = []

    def begin(copy):
        copy.start()
        sent.append(copy)

    def token_copy(role, c):
        rows = piece(role, c)
        if role == NEAR:
            origin, cols = near_rows.at[rows], half_cols(t)
        else:
            origin, cols = cross_rows.at[role - INNER, rows], f_cols(t)
        slot = slot_there[role]
        return pltpu.make_async_remote_copy(
            src_ref=origin,
            dst_ref=toks.at[slot, rows, cols],
            send_sem=zt.at[0, role, c],
            recv_sem=zt.at[1, slot, c],
            device_id={"ep": peer[role]},
            device_id_type=MESH,
        )

    def token_arrival(slot, c):
        rows = piece(slot, c)
        cols = half_cols(t) if slot == NEAR else f_cols(t)
        view = toks.at[slot, rows, cols]
        return pltpu.make_async_remote_copy(
            src_ref=view,
            dst_ref=view,
            send_sem=zt.at[0, slot, c],
            recv_sem=zt.at[1, slot, c],
            device_id={"ep": peer[slot]},
            device_id_type=MESH,
        )

    def shared(view, sems, slot, c, target):
        return pltpu.make_async_remote_copy(
            src_ref=view,
            dst_ref=view,
            send_sem=sems.at[0, slot, c],
            recv_sem=sems.at[1, slot, c],
            device_id={"tp": target},
            device_id_type=MESH,
        )

    def tok_view(slot, c, owner):
        cols = half_cols(owner) if slot == NEAR else f_cols(owner)
        return toks.at[slot, piece(slot, c), cols]

    def hid_view(slot, c, owner):
        return hid.at[slot, piece(slot, c), h_cols(owner)]

    def result_copy(slot, c):
        rows = piece(slot, c)
        there = slot_there[slot]
        return pltpu.make_async_remote_copy(
            src_ref=res.at[slot, rows],
            dst_ref=back.at[there, rows],
            send_sem=rz.at[0, slot, c],
            recv_sem=rz.at[1, there, c],
            device_id={"ep": peer[slot]},
            device_id_type=MESH,
        )

    def result_arrival(role, c):
        view = back.at[role, piece(role, c)]
        return pltpu.make_async_remote_copy(
            src_ref=view,
            dst_ref=view,
            send_sem=rz.at[0, role, c],
            recv_sem=rz.at[1, role, c],
            device_id={"ep": peer[role]},
            device_id_type=MESH,
        )

    def dispatch(role, c):
        size = capacity // PARTS[role]
        pick = picker(peer[role], c * size, size)
        if role == NEAR:
            picked = jnp.dot(pick, normed[:, half_cols(t)], preferred_element_type=jnp.float32)
            near_rows[piece(role, c), :] = picked.astype(jnp.bfloat16)
        else:
            picked = jnp.dot(pick, normed[:, f_cols(t)], preferred_element_type=jnp.float32)
            cross_rows[role - INNER, piece(role, c), :] = picked.astype(jnp.bfloat16)
        begin(token_copy(role, c))

    def first_matmul(slot, c):
        rows = piece(slot, c)
        for start in range(0, width, 256):
            size = min(256, width - start)
            value = jnp.dot(
                toks[slot, rows, :],
                up[:, start : start + size],
                preferred_element_type=jnp.float32,
            )
            value = value * jax.nn.sigmoid(value)
            cols = pl.ds(pl.multiple_of(t * width + start, 128), size)
            hid[slot, rows, cols] = value.astype(jnp.bfloat16)
        begin(shared(hid_view(slot, c, t), hx, slot, c, across))
        begin(shared(hid_view(slot, c, t), hm, slot, c, mate))

    def own_tokens(_, c):
        size = capacity // PARTS[OWN]
        mine = picker(e, c * size, size)
        for q in range(4):
            cols = slice(q * part, (q + 1) * part)
            picked = jnp.dot(mine, normed[:, cols], preferred_element_type=jnp.float32)
            toks[OWN, piece(OWN, c), cols] = picked.astype(jnp.bfloat16)
        if "up" not in waited:
            load_up.wait()
            waited.append("up")
        first_matmul(OWN, c)

    def spread(slot, c):
        token_arrival(slot, c).wait_recv()
        begin(shared(tok_view(slot, c, t), tm, slot, c, mate))
        if slot != NEAR:
            begin(shared(tok_view(slot, c, t), tx, slot, c, across))

    def forward(slot, c):
        if slot != NEAR:
            shared(tok_view(slot, c, across), tx, slot, c, across).wait_recv()
            begin(shared(tok_view(slot, c, across), tf, slot, c, mate))

    def hidden_block(slot, c):
        shared(tok_view(slot, c, mate), tm, slot, c, mate).wait_recv()
        if slot != NEAR:
            shared(tok_view(slot, c, far), tf, slot, c, mate).wait_recv()
        first_matmul(slot, c)

    def k_dot(slot, rows, first_row, size):
        cols = pl.ds(pl.multiple_of(first_row, 128), size)
        return jnp.dot(hid[slot, rows, cols], down[cols, :], preferred_element_type=jnp.float32)

    def gather_block(slot, c):
        rows = piece(slot, c)
        shared(hid_view(slot, c, across), hx, slot, c, across).wait_recv()
        begin(shared(hid_view(slot, c, across), hf, slot, c, mate))
        shared(hid_view(slot, c, mate), hm, slot, c, mate).wait_recv()
        if "down" not in waited:
            load_down.wait()
            waited.append("down")
        local = k_dot(slot, rows, (t // 2) * 2 * width, 2 * width)
        acc[slot, rows, :] = local + k_dot(slot, rows, across * width, width)

    def finish_block(slot, c):
        rows = piece(slot, c)
        shared(hid_view(slot, c, far), hf, slot, c, mate).wait_recv()
        res[slot, rows, :] = (acc[slot, rows, :] + k_dot(slot, rows, far * width, width)).astype(
            jnp.bfloat16
        )
        if slot != OWN:
            begin(result_copy(slot, c))

    blocks, size_w = carry_w_ref.shape[0], carry_w_ref.shape[1]

    def gate(w_ref, conv_half):
        whole = jnp.zeros((channels, channels), jnp.float32)
        for b in range(blocks):
            tall = (
                lax.broadcasted_iota(jnp.int32, (channels, size_w), 0)
                == lax.broadcasted_iota(jnp.int32, (channels, size_w), 1) + b * size_w
            )
            wide = (
                lax.broadcasted_iota(jnp.int32, (size_w, channels), 1)
                == lax.broadcasted_iota(jnp.int32, (size_w, channels), 0) + b * size_w
            )
            right = jnp.dot(
                w_ref[b],
                wide.astype(jnp.float32).astype(jnp.bfloat16),
                preferred_element_type=jnp.float32,
            ).astype(jnp.bfloat16)
            whole = whole + jnp.dot(
                tall.astype(jnp.float32).astype(jnp.bfloat16),
                right,
                preferred_element_type=jnp.float32,
            )
        return jax.nn.sigmoid(
            jnp.dot(conv_half, whole.astype(jnp.bfloat16), preferred_element_type=jnp.float32)
        )

    def carry_copy(j):
        return remote(carry_out, carry_in.at[j], carry_sems, j, ep=(e + n - j) % n)

    def scan_local():
        send_halo.wait_recv()
        padded[0:HALO, :] = jnp.where(e > 0, halo[...].astype(jnp.float32), 0.0)
        taps = taps_ref[...].astype(jnp.float32)
        conv = jnp.zeros((length, channels), jnp.float32)
        for k in range(CONV):
            lead = HALO - (CONV - 1) + k
            conv = conv + padded[lead : lead + length, :] * taps[k : k + 1, :]
        conv_half = conv.astype(jnp.bfloat16)
        conv_buf[...] = conv
        lane = -lane_ref[...].reshape(1, channels)
        soft = jnp.maximum(lane, 0.0) + jnp.log1p(jnp.exp(-jnp.abs(lane)))
        fade = -8.0 * gate(carry_w_ref, conv_half) * soft + as_column(jump_ref[...])
        state = jnp.sqrt(one_minus_exp(2.0 * fade)) * gate(entry_w_ref, conv_half) * conv_buf[...]
        decay = jnp.exp(fade)
        place = lax.broadcasted_iota(jnp.int32, (length, channels), 0)
        shift = 1
        while shift < length:
            older_decay = jnp.where(place < shift, 1.0, pltpu.roll(decay, shift, 0))
            older_state = jnp.where(place < shift, 0.0, pltpu.roll(state, shift, 0))
            state = decay * older_state + state
            decay = decay * older_decay
            shift *= 2
        decay_buf[...] = decay
        state_buf[...] = state
        carry_out[0:8, :] = jnp.broadcast_to(decay[length - 1 : length, :], (8, channels))
        carry_out[8:16, :] = jnp.broadcast_to(state[length - 1 : length, :], (8, channels))
        for j in range(1, n):
            begin(carry_copy(j))

    def scan_finish():
        entering = jnp.zeros((1, channels), jnp.float32)
        for j in range(1, n):
            carry_copy(j).wait_recv()
        for origin in range(n - 1):
            slot = (origin + n - e) % n
            slot = jnp.where(slot == 0, 1, slot)
            early = carry_in[slot]
            after = early[0:1, :] * entering + early[8:9, :]
            entering = jnp.where(origin < e, after, entering)
        gelu_in = valve_ref[...].astype(jnp.float32)
        inner = 0.7978845608028654 * (gelu_in + 0.044715 * (gelu_in * gelu_in * gelu_in))
        gelu = gelu_in * (0.5 * (1.0 + jnp.tanh(inner)))
        final = (state_buf[...] + decay_buf[...] * entering).T
        scan_out[...] = (final * gelu).astype(jnp.bfloat16)

    def plan_combine():
        first_col, second_col = as_column(first), as_column(second)
        scores = score_ref[...]
        first_weight = jax.nn.sigmoid(as_column(scores[0:1, :] - scores[1:2, :]))
        slots = lax.broadcasted_iota(jnp.int32, (tokens, capacity), 1).astype(jnp.float32)
        for role in (OWN, NEAR, INNER, OUTER):
            expert = peer.get(role, e)
            number = expert.astype(jnp.float32)
            rank_col = as_column(rank_rows[pl.ds(expert, 1), :])
            chosen[role] = (slots == rank_col).astype(jnp.float32).astype(jnp.bfloat16)
            weight = jnp.where(first_col == number, first_weight, 0.0) + jnp.where(
                second_col == number, 1.0 - first_weight, 0.0
            )
            share[role] = jnp.broadcast_to(weight, (tokens, 128))

    added = []

    def combine(role):
        if role != OWN:
            for c in range(PARTS[role]):
                result_arrival(role, c).wait_recv()
        source = res[OWN] if role == OWN else back[role]
        term = jnp.dot(chosen[role], source, preferred_element_type=jnp.float32)
        term = term * jnp.tile(share[role], (1, out_width // 128))
        if added:
            term = total[...] + term
        added.append(role)
        if len(added) == n:
            moe_out[...] = term.astype(jnp.bfloat16)
        else:
            total[...] = term

    tasks = {
        "D": dispatch,
        "P": own_tokens,
        "T": spread,
        "F": forward,
        "M": hidden_block,
        "G": gather_block,
        "S": finish_block,
    }
    for name in ORDER:
        with jax.named_scope(name):
            if name == "A":
                scan_local()
            elif name == "B":
                scan_finish()
                plan_combine()
            elif name[0] == "C":
                combine(int(name[1]))
            else:
                tasks[name[0]](int(name[1]), int(name[2]) - 1)

    with jax.named_scope("drain"):
        for copy in sent:
            copy.wait_send()


def slots_per_expert(tokens, top_count, experts, tp_size):
    return tp_size * ((3 * tokens * top_count + 2 * experts * tp_size - 1) // (2 * experts * tp_size))


def fused(*arrays):
    (scan, valve, taps, carry_w, entry_w, lane, jump, tok, gain, routes, scores, up, down) = arrays
    n = lax.axis_size("ep")
    length, channels = scan.shape
    tokens, features = tok.shape
    width, out_width = up.shape[2], down.shape[2]
    units = down.shape[1]
    capacity = slots_per_expert(tokens, routes.shape[1], n, lax.axis_size("tp"))
    half, full = jnp.bfloat16, jnp.float32
    vmem = pl.BlockSpec(memory_space=pltpu.VMEM)
    hbm = pl.BlockSpec(memory_space=pl.ANY)
    pair = pltpu.SemaphoreType.DMA((2, n))
    pieces = pltpu.SemaphoreType.DMA((2, n, max(PARTS.values())))
    turned, moe = pl.pallas_call(
        functools.partial(fused_kernel, n, capacity),
        out_shape=(
            pltpu.VMEM((channels, length), half),
            pltpu.VMEM((tokens, out_width), half),
        ),
        in_specs=[vmem] * 11 + [hbm] * 2,
        out_specs=(vmem, vmem),
        scratch_shapes=[
            pltpu.VMEM((features, width), half),
            pltpu.VMEM((units, out_width), half),
            pltpu.VMEM((tokens, features), half),
            pltpu.VMEM((-(-n // 8) * 8, tokens), full),
            pltpu.VMEM((capacity, features // 2), half),
            pltpu.VMEM((2, capacity, features // 4), half),
            pltpu.VMEM((n, capacity, features), half),
            pltpu.VMEM((n, capacity, units), half),
            pltpu.VMEM((n, capacity, out_width), half),
            pltpu.VMEM((n, capacity, out_width), half),
            pltpu.VMEM((n, capacity, out_width), full),
            pltpu.VMEM((n, tokens, capacity), half),
            pltpu.VMEM((n, tokens, 128), full),
            pltpu.VMEM((tokens, out_width), full),
            pltpu.VMEM((HALO, channels), half),
            pltpu.VMEM((length + HALO, channels), full),
            pltpu.VMEM((length, channels), full),
            pltpu.VMEM((length, channels), full),
            pltpu.VMEM((length, channels), full),
            pltpu.VMEM((16, channels), full),
            pltpu.VMEM((n, 16, channels), full),
            pltpu.VMEM((HALO, channels), half),
            pltpu.SemaphoreType.DMA((2,)),
            *([pieces] * 8),
            pltpu.SemaphoreType.DMA((2, 1)),
            pair,
        ],
        compiler_params=pltpu.CompilerParams(
            collective_id=0, has_side_effects=True, vmem_limit_bytes=56 * 1024 * 1024
        ),
    )(
        scan.T,
        valve.T,
        taps,
        carry_w,
        entry_w,
        lane,
        jump.reshape(1, -1),
        tok,
        gain.reshape(1, -1),
        routes.T,
        scores.T,
        up,
        down,
    )
    return turned.T, moe


def fits_fused(tok, routes, up, down):
    n, tp_size = lax.axis_size("ep"), lax.axis_size("tp")
    if tp_size != 4 or n != 4 or up.shape[0] != 1 or routes.shape[1] != 2:
        return False
    capacity = slots_per_expert(tok.shape[0], 2, n, tp_size)
    if capacity % 96 or tok.shape[0] % 32 or up.shape[2] % 128 or down.shape[2] % 256:
        return False
    held = n * capacity * (tok.shape[1] + down.shape[1] + 4 * down.shape[2])
    return 2 * (held + up.size + down.size + 3 * tok.size) < 44 * 1024 * 1024


def on_device(
    scan_branch_source,
    valve_branch_source,
    stencil_factors,
    carry_valve_matrix,
    entry_valve_matrix,
    lane_fade_param,
    jump_log_fade,
    specialist_entries,
    specialist_rms_scale,
    assigned_specialists,
    picked_route_scores,
    expand_matrix,
    contract_matrix,
):
    if fits_fused(specialist_entries, assigned_specialists, expand_matrix, contract_matrix):
        return fused(
            scan_branch_source,
            valve_branch_source,
            stencil_factors,
            carry_valve_matrix,
            entry_valve_matrix,
            lane_fade_param,
            jump_log_fade,
            specialist_entries,
            specialist_rms_scale,
            assigned_specialists,
            picked_route_scores,
            expand_matrix,
            contract_matrix,
        )
    valved_scan_target = temporal_block_part(
        scan_branch_source,
        valve_branch_source,
        stencil_factors,
        carry_valve_matrix,
        entry_valve_matrix,
        lane_fade_param,
        jump_log_fade,
    )
    moe_out = expert_part(
        specialist_entries,
        specialist_rms_scale,
        assigned_specialists,
        picked_route_scores,
        expand_matrix,
        contract_matrix,
    )
    return (valved_scan_target, moe_out)


def solution(mesh):
    placed = (
        P(("grp", "ep"), "tp"),
        P(("grp", "ep"), "tp"),
        P(None, "tp"),
        P("tp", None, None),
        P("tp", None, None),
        P("tp"),
        P(("grp", "ep")),
        P(("grp", "ep"), None),
        P(),
        P(("grp", "ep"), None),
        P(("grp", "ep"), None),
        P("ep", None, "tp"),
        P("ep", None, "tp"),
    )
    return jax.shard_map(
        on_device,
        mesh=mesh,
        in_specs=placed,
        out_specs=(P(("grp", "ep"), "tp"), P(("grp", "ep"), "tp")),
        check_vma=False,
    )
```

```python
import functools

import jax
import jax.numpy as jnp
from jax import lax
from jax.experimental import pallas as pl
from jax.experimental.pallas import tpu as pltpu
from jax.sharding import PartitionSpec as P

CONV = 4


def passed_along(block, axis, distance):
    devices = range(lax.axis_size(axis))
    route = [(i - distance, i) for i in devices if i - distance in devices]
    return lax.ppermute(block, axis, route)


def carried_in(part, axis, combine, identity):
    place = lax.axis_index(axis)
    gathered = jax.tree.map(lambda a: lax.all_gather(a, axis), part)
    state = jax.tree.map(lambda a, e: jnp.zeros_like(a) + jnp.asarray(e, a.dtype), part, identity)

    def one(step, state):
        return combine(
            state, jax.tree.map(lambda a: lax.dynamic_index_in_dim(a, step, 0, False), gathered)
        )

    return lax.fori_loop(0, place, one, state)


def chain_link(earlier, later):
    early_decay, early_state = earlier
    late_decay, late_state = later
    return (early_decay * late_decay, late_decay * early_state + late_state)


def slot_table(assigned_specialists, experts, capacity):
    flat_routes = assigned_specialists.reshape(-1)
    top_count = assigned_specialists.shape[1]
    matches = (flat_routes[:, None] == jnp.arange(experts, dtype=jnp.int32)[None, :]).astype(
        jnp.int32
    )
    before = jnp.cumsum(matches, axis=0) - matches
    slot_rank = jnp.sum(before * matches, axis=1)
    slot_index = flat_routes * capacity + slot_rank
    owner_row = jnp.arange(flat_routes.shape[0], dtype=jnp.int32) // top_count
    source = jnp.zeros((experts * capacity,), jnp.int32).at[slot_index].set(owner_row)
    filled = jnp.zeros((experts * capacity,), jnp.float32).at[slot_index].set(1.0)
    return (slot_index, source, filled)


def temporal_block_part(
    scan_branch_source,
    valve_branch_source,
    stencil_factors,
    carry_valve_matrix,
    entry_valve_matrix,
    lane_fade_param,
    jump_log_fade,
):
    length = scan_branch_source.shape[0]
    channels = scan_branch_source.shape[1]
    previous = passed_along(scan_branch_source[length - (CONV - 1) :], "ep", 1)
    padded = jnp.concatenate([previous, scan_branch_source], axis=0).astype(jnp.float32)
    tap_values = stencil_factors.astype(jnp.float32)
    conv_out = jnp.zeros((length, channels), jnp.float32)
    for offset in range(CONV):
        conv_out = conv_out + padded[offset : offset + length] * tap_values[offset]
    blocks_here = carry_valve_matrix.shape[0]
    conv_blocks = conv_out.astype(jnp.bfloat16).reshape(
        length, blocks_here, carry_valve_matrix.shape[1]
    )
    carry_valve = jax.nn.sigmoid(
        jnp.einsum(
            "tnc,ncd->tnd", conv_blocks, carry_valve_matrix, preferred_element_type=jnp.float32
        ).reshape(length, channels)
    )
    input_gate = jax.nn.sigmoid(
        jnp.einsum(
            "tnc,ncd->tnd", conv_blocks, entry_valve_matrix, preferred_element_type=jnp.float32
        ).reshape(length, channels)
    )
    fade_log_rate = (
        -8.0 * carry_valve * jax.nn.softplus(-lane_fade_param)[None, :] + jump_log_fade[:, None]
    )
    drive_term = jnp.sqrt(-jnp.expm1(2.0 * fade_log_rate)) * input_gate * conv_out
    cumulative, local_state = lax.associative_scan(
        chain_link, (jnp.exp(fade_log_rate), drive_term), axis=0
    )
    identity = (jnp.ones((channels,), jnp.float32), jnp.zeros((channels,), jnp.float32))
    entering = carried_in((cumulative[-1], local_state[-1]), "ep", chain_link, identity)
    hidden_state = local_state + cumulative * entering[1][None, :]
    return (hidden_state * jax.nn.gelu(valve_branch_source.astype(jnp.float32))).astype(
        jnp.bfloat16
    )


def expert_part(
    specialist_entries,
    specialist_rms_scale,
    assigned_specialists,
    picked_route_scores,
    expand_matrix,
    contract_matrix,
):
    ep_size = lax.axis_size("ep")
    tp_size = lax.axis_size("tp")
    exp_dev = expand_matrix.shape[0]
    experts = exp_dev * ep_size
    tokens = specialist_entries.shape[0]
    features = specialist_entries.shape[1]
    top_count = assigned_specialists.shape[1]
    capacity = tp_size * (
        (3 * tokens * top_count + 2 * experts * tp_size - 1) // (2 * experts * tp_size)
    )
    tok_rows = specialist_entries.astype(jnp.float32)
    row_mean = jnp.mean(tok_rows, axis=1, keepdims=True)
    centered = tok_rows - row_mean
    row_var = jnp.mean(centered * centered, axis=1, keepdims=True)
    normed = (centered * lax.rsqrt(row_var + 1e-05) * specialist_rms_scale[None, :]).astype(
        jnp.bfloat16
    )
    slot_index, source, filled = slot_table(assigned_specialists, experts, capacity)
    source_grid = source.reshape(experts, capacity)
    filled_grid = filled.reshape(experts, capacity)
    slice_size = capacity // tp_size
    first_slot = lax.axis_index("tp") * slice_size
    source_grid = lax.dynamic_slice_in_dim(source_grid, first_slot, slice_size, 1)
    filled_grid = lax.dynamic_slice_in_dim(filled_grid, first_slot, slice_size, 1)
    outgoing = normed[source_grid] * filled_grid[:, :, None].astype(jnp.bfloat16)
    outgoing = outgoing.reshape(ep_size, exp_dev, source_grid.shape[1], features)
    arrived = lax.all_to_all(outgoing, "ep", split_axis=0, concat_axis=0, tiled=True)
    arrived = lax.all_gather(arrived, "tp", axis=2, tiled=True)
    hidden = jax.nn.silu(
        jnp.einsum("secd,edf->secf", arrived, expand_matrix, preferred_element_type=jnp.float32)
    ).astype(jnp.bfloat16)
    column_count = contract_matrix.shape[2]
    expert_out = jnp.einsum(
        "secf,efd->secd",
        lax.all_gather(hidden, "tp", axis=3, tiled=True),
        contract_matrix,
        preferred_element_type=jnp.float32,
    ).astype(jnp.bfloat16)
    returned = lax.all_to_all(expert_out, "ep", split_axis=0, concat_axis=0, tiled=True)
    returned = returned.reshape(experts * capacity, column_count)
    picked = returned[slot_index].reshape(tokens, top_count, column_count).astype(jnp.float32)
    first_weight = jax.nn.sigmoid(picked_route_scores[:, 0] - picked_route_scores[:, 1])
    weights = jnp.stack([first_weight, 1.0 - first_weight], axis=1)
    return jnp.sum(weights[:, :, None] * picked, axis=1).astype(jnp.bfloat16)


MESH = pl.DeviceIdType.MESH
HALO = 16


def remote(src, dst, sems, index, **device):
    return pltpu.make_async_remote_copy(
        src_ref=src,
        dst_ref=dst,
        send_sem=sems.at[0, index],
        recv_sem=sems.at[1, index],
        device_id=device,
        device_id_type=MESH,
    )


def as_column(row):
    n = row.shape[1]
    same = lax.broadcasted_iota(jnp.int32, (n, n), 0) == lax.broadcasted_iota(jnp.int32, (n, n), 1)
    return jnp.sum(jnp.where(same, row, 0.0), axis=1, keepdims=True)


def one_minus_exp(x):
    near = jnp.maximum(x, -0.35)
    series = 1.0 + near * (1.0 / 8.0)
    for divisor in (7.0, 6.0, 5.0, 4.0, 3.0, 2.0):
        series = 1.0 + near * (1.0 / divisor) * series
    return jnp.where(x > -0.35, -near * series, 1.0 - jnp.exp(x))


OWN, NEAR, INNER, OUTER = 0, 1, 2, 3
PARTS = {OWN: 3, NEAR: 3, INNER: 3, OUTER: 3}
ORDER = (
    "D31", "P01", "D21", "D32", "P02", "D22", "T31", "D12", "D33", "D23", "T32", "F31",
    "T21", "M31", "T12", "F32", "D13", "T33", "M32", "T22", "A", "G31", "T23", "F33",
    "G02", "M33", "F21", "D11", "M21", "F23", "F22", "G32", "T13", "M22", "S32", "G33",
    "S31", "T11", "M23", "G01", "M12", "S33", "M11", "G21", "S02", "S21", "B", "M13",
    "G23", "G22", "P03", "S01", "S22", "G12", "S23", "S12", "G11", "S11", "G13", "S13",
    "G03", "C2", "C3", "S03", "C0", "C1",
)


def fused_kernel(
    n,
    capacity,
    scan_ref,
    valve_ref,
    taps_ref,
    carry_w_ref,
    entry_w_ref,
    lane_ref,
    jump_ref,
    tok_ref,
    gain_ref,
    route_ref,
    score_ref,
    up_hbm,
    down_hbm,
    scan_out,
    moe_out,
    up,
    down,
    normed,
    rank_rows,
    near_rows,
    cross_rows,
    toks,
    hid,
    res,
    back,
    acc,
    chosen,
    share,
    total,
    halo,
    padded,
    conv_buf,
    decay_buf,
    state_buf,
    carry_out,
    carry_in,
    halo_out,
    load_sems,
    zt,
    tx,
    tm,
    tf,
    hx,
    hm,
    hf,
    rz,
    out_sems,
    halo_sems,
    carry_sems,
):
    e = lax.axis_index("ep")
    t = lax.axis_index("tp")
    mate = t + 1 - 2 * (t % 2)
    across = (t + 2) % 4
    far = (mate + 2) % 4
    upper = e // 2
    peer = {NEAR: e + 1 - 2 * (e % 2), INNER: 2 - upper, OUTER: 3 - 3 * upper}
    cross_slot = OUTER - (e + upper) % 2
    slot_there = {NEAR: NEAR, INNER: cross_slot, OUTER: cross_slot}
    tx, tm, tf = (2, INNER, tx), (3, NEAR, tm), (4, INNER, tf)
    hx, hm, hf = (5, OWN, hx), (6, OWN, hm), (7, OWN, hf)
    tokens, features = tok_ref.shape
    part = features // 4
    width = up.shape[1]
    out_width = down.shape[1]

    def f_cols(i):
        return pl.ds(pl.multiple_of(i * part, part), part)

    def half_cols(i):
        return pl.ds(pl.multiple_of((i % 2) * 2 * part, 2 * part), 2 * part)

    def h_cols(i):
        return pl.ds(pl.multiple_of(i * width, 128), width)

    def piece(slot, c):
        size = capacity // PARTS[slot]
        return pl.ds(c * size, size)

    barrier = pltpu.get_barrier_semaphore()
    for j in range(1, n):
        pl.semaphore_signal(barrier, inc=1, device_id={"ep": (e + j) % n}, device_id_type=MESH)
    for other in (mate, across):
        pl.semaphore_signal(barrier, inc=1, device_id={"tp": other}, device_id_type=MESH)
    load_up = pltpu.make_async_copy(up_hbm.at[0], up, load_sems.at[0])
    load_down = pltpu.make_async_copy(down_hbm.at[0], down, load_sems.at[1])
    load_up.start()
    load_down.start()
    channels, length = scan_ref.shape

    with jax.named_scope("halo_prep"):
        turned = scan_ref[...].astype(jnp.float32).T
        padded[HALO:, :] = turned
        halo_out[...] = turned[length - HALO :, :].astype(jnp.bfloat16)

    rows_step = 64

    def norm_rows(i, _):
        rows = pl.ds(pl.multiple_of(i * rows_step, rows_step), rows_step)
        x = tok_ref[rows, :].astype(jnp.float32)
        centered = x - jnp.sum(x, axis=1, keepdims=True) * (1.0 / features)
        var = jnp.sum(centered * centered, axis=1, keepdims=True) * (1.0 / features)
        normed[rows, :] = (centered * lax.rsqrt(var + 1e-05) * gain_ref[...]).astype(jnp.bfloat16)
        return 0

    with jax.named_scope("norm"):
        lax.fori_loop(0, tokens // rows_step, norm_rows, 0)

    with jax.named_scope("rank"):
        routes = route_ref[...].astype(jnp.float32)
        first, second = routes[0:1, :], routes[1:2, :]
        erow = lax.broadcasted_iota(jnp.int32, (rank_rows.shape[0], tokens), 0).astype(jnp.float32)
        hit = (erow == first) | (erow == second)
        ti = lax.broadcasted_iota(jnp.int32, (tokens, tokens), 0)
        tj = lax.broadcasted_iota(jnp.int32, (tokens, tokens), 1)
        rank = jnp.dot(
            hit.astype(jnp.float32).astype(jnp.bfloat16),
            (ti < tj).astype(jnp.float32).astype(jnp.bfloat16),
            preferred_element_type=jnp.float32,
        )
        rank_rows[...] = jnp.where(hit, rank, -1.0)

    def picker(expert, start, size):
        slots = start + lax.broadcasted_iota(jnp.int32, (size, tokens), 0)
        hits = slots.astype(jnp.float32) == rank_rows[pl.ds(expert, 1), :]
        return hits.astype(jnp.float32).astype(jnp.bfloat16)

    with jax.named_scope("barrier"):
        pl.semaphore_wait(barrier, n + 1)

    send_halo = remote(halo_out, halo, halo_sems, 0, ep=(e + 1) % n)
    send_halo.start()
    sent = [send_halo]
    waited = []

    def begin(copy):
        copy.start()

    def token_copy(role, c):
        rows = piece(role, c)
        if role == NEAR:
            origin, cols = near_rows.at[rows], half_cols(t)
        else:
            origin, cols = cross_rows.at[role - INNER, rows], f_cols(t)
        slot = slot_there[role]
        return pltpu.make_async_remote_copy(
            src_ref=origin,
            dst_ref=toks.at[slot, rows, cols],
            send_sem=out_sems.at[0],
            recv_sem=zt.at[slot - 1, c],
            device_id={"ep": peer[role]},
            device_id_type=MESH,
        )

    def token_arrival(slot, c):
        rows = piece(slot, c)
        cols = half_cols(t) if slot == NEAR else f_cols(t)
        view = toks.at[slot, rows, cols]
        return pltpu.make_async_remote_copy(
            src_ref=view,
            dst_ref=view,
            send_sem=out_sems.at[0],
            recv_sem=zt.at[slot - 1, c],
            device_id={"ep": peer[slot]},
            device_id_type=MESH,
        )

    def shared(view, sems, slot, c, target):
        kind, first, sems = sems
        return pltpu.make_async_remote_copy(
            src_ref=view,
            dst_ref=view,
            send_sem=out_sems.at[kind],
            recv_sem=sems.at[slot - first, c],
            device_id={"tp": target},
            device_id_type=MESH,
        )

    def tok_view(slot, c, owner):
        cols = half_cols(owner) if slot == NEAR else f_cols(owner)
        return toks.at[slot, piece(slot, c), cols]

    def hid_view(slot, c, owner):
        return hid.at[slot, piece(slot, c), h_cols(owner)]

    def result_copy(slot, c):
        rows = piece(slot, c)
        there = slot_there[slot]
        return pltpu.make_async_remote_copy(
            src_ref=res.at[slot, rows],
            dst_ref=back.at[there, rows],
            send_sem=out_sems.at[1],
            recv_sem=rz.at[there - 1, c],
            device_id={"ep": peer[slot]},
            device_id_type=MESH,
        )

    def result_arrival(role, c):
        view = back.at[role, piece(role, c)]
        return pltpu.make_async_remote_copy(
            src_ref=view,
            dst_ref=view,
            send_sem=out_sems.at[1],
            recv_sem=rz.at[role - 1, c],
            device_id={"ep": peer[role]},
            device_id_type=MESH,
        )

    def dispatch(role, c):
        size = capacity // PARTS[role]
        pick = picker(peer[role], c * size, size)
        if role == NEAR:
            picked = jnp.dot(pick, normed[:, half_cols(t)], preferred_element_type=jnp.float32)
            near_rows[piece(role, c), :] = picked.astype(jnp.bfloat16)
        else:
            picked = jnp.dot(pick, normed[:, f_cols(t)], preferred_element_type=jnp.float32)
            cross_rows[role - INNER, piece(role, c), :] = picked.astype(jnp.bfloat16)
        begin(token_copy(role, c))

    def first_matmul(slot, c):
        rows = piece(slot, c)
        for start in range(0, width, 256):
            size = min(256, width - start)
            value = jnp.dot(
                toks[slot, rows, :],
                up[:, start : start + size],
                preferred_element_type=jnp.float32,
            )
            value = value * jax.nn.sigmoid(value)
            cols = pl.ds(pl.multiple_of(t * width + start, 128), size)
            hid[slot, rows, cols] = value.astype(jnp.bfloat16)
        begin(shared(hid_view(slot, c, t), hx, slot, c, across))
        begin(shared(hid_view(slot, c, t), hm, slot, c, mate))

    def own_tokens(_, c):
        size = capacity // PARTS[OWN]
        mine = picker(e, c * size, size)
        for q in range(4):
            cols = slice(q * part, (q + 1) * part)
            picked = jnp.dot(mine, normed[:, cols], preferred_element_type=jnp.float32)
            toks[OWN, piece(OWN, c), cols] = picked.astype(jnp.bfloat16)
        if "up" not in waited:
            load_up.wait()
            waited.append("up")
        first_matmul(OWN, c)

    def spread(slot, c):
        token_arrival(slot, c).wait_recv()
        begin(shared(tok_view(slot, c, t), tm, slot, c, mate))
        if slot != NEAR:
            begin(shared(tok_view(slot, c, t), tx, slot, c, across))

    def forward(slot, c):
        if slot != NEAR:
            shared(tok_view(slot, c, across), tx, slot, c, across).wait_recv()
            begin(shared(tok_view(slot, c, across), tf, slot, c, mate))

    def hidden_block(slot, c):
        shared(tok_view(slot, c, mate), tm, slot, c, mate).wait_recv()
        if slot != NEAR:
            shared(tok_view(slot, c, far), tf, slot, c, mate).wait_recv()
        first_matmul(slot, c)

    def k_dot(slot, rows, first_row, size):
        cols = pl.ds(pl.multiple_of(first_row, 128), size)
        return jnp.dot(hid[slot, rows, cols], down[cols, :], preferred_element_type=jnp.float32)

    def gather_block(slot, c):
        rows = piece(slot, c)
        shared(hid_view(slot, c, across), hx, slot, c, across).wait_recv()
        begin(shared(hid_view(slot, c, across), hf, slot, c, mate))
        shared(hid_view(slot, c, mate), hm, slot, c, mate).wait_recv()
        if "down" not in waited:
            load_down.wait()
            waited.append("down")
        local = k_dot(slot, rows, (t // 2) * 2 * width, 2 * width)
        acc[slot, rows, :] = local + k_dot(slot, rows, across * width, width)

    def finish_block(slot, c):
        rows = piece(slot, c)
        shared(hid_view(slot, c, far), hf, slot, c, mate).wait_recv()
        res[slot, rows, :] = (acc[slot, rows, :] + k_dot(slot, rows, far * width, width)).astype(
            jnp.bfloat16
        )
        if slot != OWN:
            begin(result_copy(slot, c))

    blocks, size_w = carry_w_ref.shape[0], carry_w_ref.shape[1]

    def gate(w_ref, conv_half):
        whole = jnp.zeros((channels, channels), jnp.float32)
        for b in range(blocks):
            tall = (
                lax.broadcasted_iota(jnp.int32, (channels, size_w), 0)
                == lax.broadcasted_iota(jnp.int32, (channels, size_w), 1) + b * size_w
            )
            wide = (
                lax.broadcasted_iota(jnp.int32, (size_w, channels), 1)
                == lax.broadcasted_iota(jnp.int32, (size_w, channels), 0) + b * size_w
            )
            right = jnp.dot(
                w_ref[b],
                wide.astype(jnp.float32).astype(jnp.bfloat16),
                preferred_element_type=jnp.float32,
            ).astype(jnp.bfloat16)
            whole = whole + jnp.dot(
                tall.astype(jnp.float32).astype(jnp.bfloat16),
                right,
                preferred_element_type=jnp.float32,
            )
        return jax.nn.sigmoid(
            jnp.dot(conv_half, whole.astype(jnp.bfloat16), preferred_element_type=jnp.float32)
        )

    def carry_copy(j):
        return remote(carry_out, carry_in.at[j], carry_sems, j, ep=(e + n - j) % n)

    def scan_local():
        send_halo.wait_recv()
        padded[0:HALO, :] = jnp.where(e > 0, halo[...].astype(jnp.float32), 0.0)
        taps = taps_ref[...].astype(jnp.float32)
        conv = jnp.zeros((length, channels), jnp.float32)
        for k in range(CONV):
            lead = HALO - (CONV - 1) + k
            conv = conv + padded[lead : lead + length, :] * taps[k : k + 1, :]
        conv_half = conv.astype(jnp.bfloat16)
        conv_buf[...] = conv
        lane = -lane_ref[...].reshape(1, channels)
        soft = jnp.maximum(lane, 0.0) + jnp.log1p(jnp.exp(-jnp.abs(lane)))
        fade = -8.0 * gate(carry_w_ref, conv_half) * soft + as_column(jump_ref[...])
        state = jnp.sqrt(one_minus_exp(2.0 * fade)) * gate(entry_w_ref, conv_half) * conv_buf[...]
        decay = jnp.exp(fade)
        place = lax.broadcasted_iota(jnp.int32, (length, channels), 0)
        shift = 1
        while shift < length:
            older_decay = jnp.where(place < shift, 1.0, pltpu.roll(decay, shift, 0))
            older_state = jnp.where(place < shift, 0.0, pltpu.roll(state, shift, 0))
            state = decay * older_state + state
            decay = decay * older_decay
            shift *= 2
        decay_buf[...] = decay
        state_buf[...] = state
        carry_out[0:8, :] = jnp.broadcast_to(decay[length - 1 : length, :], (8, channels))
        carry_out[8:16, :] = jnp.broadcast_to(state[length - 1 : length, :], (8, channels))
        for j in range(1, n):
            begin(carry_copy(j))
            sent.append(carry_copy(j))

    def scan_finish():
        entering = jnp.zeros((1, channels), jnp.float32)
        for j in range(1, n):
            carry_copy(j).wait_recv()
        for origin in range(n - 1):
            slot = (origin + n - e) % n
            slot = jnp.where(slot == 0, 1, slot)
            early = carry_in[slot]
            after = early[0:1, :] * entering + early[8:9, :]
            entering = jnp.where(origin < e, after, entering)
        gelu_in = valve_ref[...].astype(jnp.float32)
        inner = 0.7978845608028654 * (gelu_in + 0.044715 * (gelu_in * gelu_in * gelu_in))
        gelu = gelu_in * (0.5 * (1.0 + jnp.tanh(inner)))
        final = (state_buf[...] + decay_buf[...] * entering).T
        scan_out[...] = (final * gelu).astype(jnp.bfloat16)

    def plan_combine():
        first_col, second_col = as_column(first), as_column(second)
        scores = score_ref[...]
        first_weight = jax.nn.sigmoid(as_column(scores[0:1, :] - scores[1:2, :]))
        slots = lax.broadcasted_iota(jnp.int32, (tokens, capacity), 1).astype(jnp.float32)
        for role in (OWN, NEAR, INNER, OUTER):
            expert = peer.get(role, e)
            number = expert.astype(jnp.float32)
            rank_col = as_column(rank_rows[pl.ds(expert, 1), :])
            chosen[role] = (slots == rank_col).astype(jnp.float32).astype(jnp.bfloat16)
            weight = jnp.where(first_col == number, first_weight, 0.0) + jnp.where(
                second_col == number, 1.0 - first_weight, 0.0
            )
            share[role] = jnp.broadcast_to(weight, (tokens, 128))

    added = []

    def combine(role):
        if role != OWN:
            for c in range(PARTS[role]):
                result_arrival(role, c).wait_recv()
        source = res[OWN] if role == OWN else back[role]
        term = jnp.dot(chosen[role], source, preferred_element_type=jnp.float32)
        term = term * jnp.tile(share[role], (1, out_width // 128))
        if added:
            term = total[...] + term
        added.append(role)
        if len(added) == n:
            moe_out[...] = term.astype(jnp.bfloat16)
        else:
            total[...] = term

    tasks = {
        "D": dispatch,
        "P": own_tokens,
        "T": spread,
        "F": forward,
        "M": hidden_block,
        "G": gather_block,
        "S": finish_block,
    }
    for name in ORDER:
        with jax.named_scope(name):
            if name == "A":
                scan_local()
            elif name == "B":
                scan_finish()
                plan_combine()
            elif name[0] == "C":
                combine(int(name[1]))
            else:
                tasks[name[0]](int(name[1]), int(name[2]) - 1)

    def sent_all(kind, view):
        pltpu.make_async_remote_copy(
            src_ref=view,
            dst_ref=view,
            send_sem=out_sems.at[kind],
            recv_sem=out_sems.at[kind],
            device_id={"tp": mate},
            device_id_type=MESH,
        ).wait_send()

    with jax.named_scope("drain"):
        sent_all(0, toks.at[:, :, f_cols(t)])
        sent_all(1, res.at[pl.ds(NEAR, n - 1)])
        sent_all(2, toks.at[pl.ds(INNER, 2), :, f_cols(t)])
        sent_all(3, toks.at[:, :, f_cols(t)])
        sent_all(4, toks.at[pl.ds(INNER, 2), :, f_cols(t)])
        for kind in (5, 6, 7):
            sent_all(kind, hid.at[:, :, h_cols(t)])
        for copy in sent:
            copy.wait_send()


def slots_per_expert(tokens, top_count, experts, tp_size):
    return tp_size * ((3 * tokens * top_count + 2 * experts * tp_size - 1) // (2 * experts * tp_size))


def fused(*arrays):
    (scan, valve, taps, carry_w, entry_w, lane, jump, tok, gain, routes, scores, up, down) = arrays
    n = lax.axis_size("ep")
    length, channels = scan.shape
    tokens, features = tok.shape
    width, out_width = up.shape[2], down.shape[2]
    units = down.shape[1]
    capacity = slots_per_expert(tokens, routes.shape[1], n, lax.axis_size("tp"))
    half, full = jnp.bfloat16, jnp.float32
    vmem = pl.BlockSpec(memory_space=pltpu.VMEM)
    hbm = pl.BlockSpec(memory_space=pl.ANY)
    pair = pltpu.SemaphoreType.DMA((2, n))
    most = max(PARTS.values())
    two, three, four = (pltpu.SemaphoreType.DMA((k, most)) for k in (2, 3, 4))
    turned, moe = pl.pallas_call(
        functools.partial(fused_kernel, n, capacity),
        out_shape=(
            pltpu.VMEM((channels, length), half),
            pltpu.VMEM((tokens, out_width), half),
        ),
        in_specs=[vmem] * 11 + [hbm] * 2,
        out_specs=(vmem, vmem),
        scratch_shapes=[
            pltpu.VMEM((features, width), half),
            pltpu.VMEM((units, out_width), half),
            pltpu.VMEM((tokens, features), half),
            pltpu.VMEM((-(-n // 8) * 8, tokens), full),
            pltpu.VMEM((capacity, features // 2), half),
            pltpu.VMEM((2, capacity, features // 4), half),
            pltpu.VMEM((n, capacity, features), half),
            pltpu.VMEM((n, capacity, units), half),
            pltpu.VMEM((n, capacity, out_width), half),
            pltpu.VMEM((n, capacity, out_width), half),
            pltpu.VMEM((n, capacity, out_width), full),
            pltpu.VMEM((n, tokens, capacity), half),
            pltpu.VMEM((n, tokens, 128), full),
            pltpu.VMEM((tokens, out_width), full),
            pltpu.VMEM((HALO, channels), half),
            pltpu.VMEM((length + HALO, channels), full),
            pltpu.VMEM((length, channels), full),
            pltpu.VMEM((length, channels), full),
            pltpu.VMEM((length, channels), full),
            pltpu.VMEM((16, channels), full),
            pltpu.VMEM((n, 16, channels), full),
            pltpu.VMEM((HALO, channels), half),
            pltpu.SemaphoreType.DMA((2,)),
            three,
            two,
            three,
            two,
            *([four] * 3),
            three,
            pltpu.SemaphoreType.DMA((8,)),
            pltpu.SemaphoreType.DMA((2, 1)),
            pair,
        ],
        compiler_params=pltpu.CompilerParams(
            collective_id=0, has_side_effects=True, vmem_limit_bytes=56 * 1024 * 1024
        ),
    )(
        scan.T,
        valve.T,
        taps,
        carry_w,
        entry_w,
        lane,
        jump.reshape(1, -1),
        tok,
        gain.reshape(1, -1),
        routes.T,
        scores.T,
        up,
        down,
    )
    return turned.T, moe


def fits_fused(tok, routes, up, down):
    n, tp_size = lax.axis_size("ep"), lax.axis_size("tp")
    if tp_size != 4 or n != 4 or up.shape[0] != 1 or routes.shape[1] != 2:
        return False
    capacity = slots_per_expert(tok.shape[0], 2, n, tp_size)
    if capacity % 96 or tok.shape[0] % 32 or up.shape[2] % 128 or down.shape[2] % 256:
        return False
    held = n * capacity * (tok.shape[1] + down.shape[1] + 4 * down.shape[2])
    return 2 * (held + up.size + down.size + 3 * tok.size) < 44 * 1024 * 1024


def on_device(
    scan_branch_source,
    valve_branch_source,
    stencil_factors,
    carry_valve_matrix,
    entry_valve_matrix,
    lane_fade_param,
    jump_log_fade,
    specialist_entries,
    specialist_rms_scale,
    assigned_specialists,
    picked_route_scores,
    expand_matrix,
    contract_matrix,
):
    if fits_fused(specialist_entries, assigned_specialists, expand_matrix, contract_matrix):
        return fused(
            scan_branch_source,
            valve_branch_source,
            stencil_factors,
            carry_valve_matrix,
            entry_valve_matrix,
            lane_fade_param,
            jump_log_fade,
            specialist_entries,
            specialist_rms_scale,
            assigned_specialists,
            picked_route_scores,
            expand_matrix,
            contract_matrix,
        )
    valved_scan_target = temporal_block_part(
        scan_branch_source,
        valve_branch_source,
        stencil_factors,
        carry_valve_matrix,
        entry_valve_matrix,
        lane_fade_param,
        jump_log_fade,
    )
    moe_out = expert_part(
        specialist_entries,
        specialist_rms_scale,
        assigned_specialists,
        picked_route_scores,
        expand_matrix,
        contract_matrix,
    )
    return (valved_scan_target, moe_out)


def solution(mesh):
    placed = (
        P(("grp", "ep"), "tp"),
        P(("grp", "ep"), "tp"),
        P(None, "tp"),
        P("tp", None, None),
        P("tp", None, None),
        P("tp"),
        P(("grp", "ep")),
        P(("grp", "ep"), None),
        P(),
        P(("grp", "ep"), None),
        P(("grp", "ep"), None),
        P("ep", None, "tp"),
        P("ep", None, "tp"),
    )
    return jax.shard_map(
        on_device,
        mesh=mesh,
        in_specs=placed,
        out_specs=(P(("grp", "ep"), "tp"), P(("grp", "ep"), "tp")),
        check_vma=False,
    )
```

```python
import functools

import jax
import jax.numpy as jnp
from jax import lax
from jax.experimental import pallas as pl
from jax.experimental.pallas import tpu as pltpu
from jax.sharding import PartitionSpec as P

CONV = 4


def passed_along(block, axis, distance):
    devices = range(lax.axis_size(axis))
    route = [(i - distance, i) for i in devices if i - distance in devices]
    return lax.ppermute(block, axis, route)


def carried_in(part, axis, combine, identity):
    place = lax.axis_index(axis)
    gathered = jax.tree.map(lambda a: lax.all_gather(a, axis), part)
    state = jax.tree.map(lambda a, e: jnp.zeros_like(a) + jnp.asarray(e, a.dtype), part, identity)

    def one(step, state):
        return combine(
            state, jax.tree.map(lambda a: lax.dynamic_index_in_dim(a, step, 0, False), gathered)
        )

    return lax.fori_loop(0, place, one, state)


def chain_link(earlier, later):
    early_decay, early_state = earlier
    late_decay, late_state = later
    return (early_decay * late_decay, late_decay * early_state + late_state)


def slot_table(assigned_specialists, experts, capacity):
    flat_routes = assigned_specialists.reshape(-1)
    top_count = assigned_specialists.shape[1]
    matches = (flat_routes[:, None] == jnp.arange(experts, dtype=jnp.int32)[None, :]).astype(
        jnp.int32
    )
    before = jnp.cumsum(matches, axis=0) - matches
    slot_rank = jnp.sum(before * matches, axis=1)
    slot_index = flat_routes * capacity + slot_rank
    owner_row = jnp.arange(flat_routes.shape[0], dtype=jnp.int32) // top_count
    source = jnp.zeros((experts * capacity,), jnp.int32).at[slot_index].set(owner_row)
    filled = jnp.zeros((experts * capacity,), jnp.float32).at[slot_index].set(1.0)
    return (slot_index, source, filled)


def temporal_block_part(
    scan_branch_source,
    valve_branch_source,
    stencil_factors,
    carry_valve_matrix,
    entry_valve_matrix,
    lane_fade_param,
    jump_log_fade,
):
    length = scan_branch_source.shape[0]
    channels = scan_branch_source.shape[1]
    previous = passed_along(scan_branch_source[length - (CONV - 1) :], "ep", 1)
    padded = jnp.concatenate([previous, scan_branch_source], axis=0).astype(jnp.float32)
    tap_values = stencil_factors.astype(jnp.float32)
    conv_out = jnp.zeros((length, channels), jnp.float32)
    for offset in range(CONV):
        conv_out = conv_out + padded[offset : offset + length] * tap_values[offset]
    blocks_here = carry_valve_matrix.shape[0]
    conv_blocks = conv_out.astype(jnp.bfloat16).reshape(
        length, blocks_here, carry_valve_matrix.shape[1]
    )
    carry_valve = jax.nn.sigmoid(
        jnp.einsum(
            "tnc,ncd->tnd", conv_blocks, carry_valve_matrix, preferred_element_type=jnp.float32
        ).reshape(length, channels)
    )
    input_gate = jax.nn.sigmoid(
        jnp.einsum(
            "tnc,ncd->tnd", conv_blocks, entry_valve_matrix, preferred_element_type=jnp.float32
        ).reshape(length, channels)
    )
    fade_log_rate = (
        -8.0 * carry_valve * jax.nn.softplus(-lane_fade_param)[None, :] + jump_log_fade[:, None]
    )
    drive_term = jnp.sqrt(-jnp.expm1(2.0 * fade_log_rate)) * input_gate * conv_out
    cumulative, local_state = lax.associative_scan(
        chain_link, (jnp.exp(fade_log_rate), drive_term), axis=0
    )
    identity = (jnp.ones((channels,), jnp.float32), jnp.zeros((channels,), jnp.float32))
    entering = carried_in((cumulative[-1], local_state[-1]), "ep", chain_link, identity)
    hidden_state = local_state + cumulative * entering[1][None, :]
    return (hidden_state * jax.nn.gelu(valve_branch_source.astype(jnp.float32))).astype(
        jnp.bfloat16
    )


def expert_part(
    specialist_entries,
    specialist_rms_scale,
    assigned_specialists,
    picked_route_scores,
    expand_matrix,
    contract_matrix,
):
    ep_size = lax.axis_size("ep")
    tp_size = lax.axis_size("tp")
    exp_dev = expand_matrix.shape[0]
    experts = exp_dev * ep_size
    tokens = specialist_entries.shape[0]
    features = specialist_entries.shape[1]
    top_count = assigned_specialists.shape[1]
    capacity = tp_size * (
        (3 * tokens * top_count + 2 * experts * tp_size - 1) // (2 * experts * tp_size)
    )
    tok_rows = specialist_entries.astype(jnp.float32)
    row_mean = jnp.mean(tok_rows, axis=1, keepdims=True)
    centered = tok_rows - row_mean
    row_var = jnp.mean(centered * centered, axis=1, keepdims=True)
    normed = (centered * lax.rsqrt(row_var + 1e-05) * specialist_rms_scale[None, :]).astype(
        jnp.bfloat16
    )
    slot_index, source, filled = slot_table(assigned_specialists, experts, capacity)
    source_grid = source.reshape(experts, capacity)
    filled_grid = filled.reshape(experts, capacity)
    slice_size = capacity // tp_size
    first_slot = lax.axis_index("tp") * slice_size
    source_grid = lax.dynamic_slice_in_dim(source_grid, first_slot, slice_size, 1)
    filled_grid = lax.dynamic_slice_in_dim(filled_grid, first_slot, slice_size, 1)
    outgoing = normed[source_grid] * filled_grid[:, :, None].astype(jnp.bfloat16)
    outgoing = outgoing.reshape(ep_size, exp_dev, source_grid.shape[1], features)
    arrived = lax.all_to_all(outgoing, "ep", split_axis=0, concat_axis=0, tiled=True)
    arrived = lax.all_gather(arrived, "tp", axis=2, tiled=True)
    hidden = jax.nn.silu(
        jnp.einsum("secd,edf->secf", arrived, expand_matrix, preferred_element_type=jnp.float32)
    ).astype(jnp.bfloat16)
    column_count = contract_matrix.shape[2]
    expert_out = jnp.einsum(
        "secf,efd->secd",
        lax.all_gather(hidden, "tp", axis=3, tiled=True),
        contract_matrix,
        preferred_element_type=jnp.float32,
    ).astype(jnp.bfloat16)
    returned = lax.all_to_all(expert_out, "ep", split_axis=0, concat_axis=0, tiled=True)
    returned = returned.reshape(experts * capacity, column_count)
    picked = returned[slot_index].reshape(tokens, top_count, column_count).astype(jnp.float32)
    first_weight = jax.nn.sigmoid(picked_route_scores[:, 0] - picked_route_scores[:, 1])
    weights = jnp.stack([first_weight, 1.0 - first_weight], axis=1)
    return jnp.sum(weights[:, :, None] * picked, axis=1).astype(jnp.bfloat16)


MESH = pl.DeviceIdType.MESH
HALO = 16


def remote(src, dst, sems, index, **device):
    return pltpu.make_async_remote_copy(
        src_ref=src,
        dst_ref=dst,
        send_sem=sems.at[0, index],
        recv_sem=sems.at[1, index],
        device_id=device,
        device_id_type=MESH,
    )


def as_column(row):
    n = row.shape[1]
    same = lax.broadcasted_iota(jnp.int32, (n, n), 0) == lax.broadcasted_iota(jnp.int32, (n, n), 1)
    return jnp.sum(jnp.where(same, row, 0.0), axis=1, keepdims=True)


def one_minus_exp(x):
    near = jnp.maximum(x, -0.35)
    series = 1.0 + near * (1.0 / 8.0)
    for divisor in (7.0, 6.0, 5.0, 4.0, 3.0, 2.0):
        series = 1.0 + near * (1.0 / divisor) * series
    return jnp.where(x > -0.35, -near * series, 1.0 - jnp.exp(x))


OWN, NEAR, INNER, OUTER = 0, 1, 2, 3
PARTS = {OWN: 3, NEAR: 3, INNER: 3, OUTER: 3}
ORDER = (
    "D31", "P01", "D21", "D32", "P02", "D22", "H", "T31", "D12", "D33", "D23", "T32",
    "F31", "T21", "M31", "T12", "F32", "D13", "T33", "M32", "T22", "A", "G31", "T23",
    "F33", "G02", "M33", "F21", "D11", "M21", "F23", "F22", "G32", "T13", "M22", "S32",
    "G33", "S31", "T11", "M23", "G01", "M12", "S33", "M11", "G21", "S02", "S21", "B",
    "M13", "G23", "G22", "P03", "S01", "S22", "G12", "S23", "S12", "G11", "S11", "G13",
    "S13", "G03", "C2", "C3", "S03", "C0", "C1",
)


def fused_kernel(
    n,
    capacity,
    scan_hbm,
    valve_hbm,
    taps_hbm,
    carry_w_hbm,
    entry_w_hbm,
    lane_hbm,
    jump_hbm,
    tok_hbm,
    gain_hbm,
    route_hbm,
    score_hbm,
    up_hbm,
    down_hbm,
    scan_out,
    moe_out,
    scan_ref,
    valve_ref,
    taps_ref,
    carry_w_ref,
    entry_w_ref,
    lane_ref,
    jump_ref,
    tok_ref,
    gain_ref,
    route_ref,
    score_ref,
    up,
    down,
    normed,
    rank_rows,
    near_rows,
    cross_rows,
    toks,
    hid,
    res,
    back,
    acc,
    chosen,
    share,
    total,
    halo,
    padded,
    conv_buf,
    decay_buf,
    state_buf,
    carry_out,
    carry_in,
    halo_out,
    load_sems,
    zt,
    tx,
    tm,
    tf,
    hx,
    hm,
    hf,
    rz,
    out_sems,
    halo_sems,
    carry_sems,
):
    e = lax.axis_index("ep")
    t = lax.axis_index("tp")
    mate = t + 1 - 2 * (t % 2)
    across = (t + 2) % 4
    far = (mate + 2) % 4
    upper = e // 2
    peer = {NEAR: e + 1 - 2 * (e % 2), INNER: 2 - upper, OUTER: 3 - 3 * upper}
    cross_slot = OUTER - (e + upper) % 2
    slot_there = {NEAR: NEAR, INNER: cross_slot, OUTER: cross_slot}
    tx, tm, tf = (2, INNER, tx), (3, NEAR, tm), (4, INNER, tf)
    hx, hm, hf = (5, OWN, hx), (6, OWN, hm), (7, OWN, hf)
    tokens, features = tok_ref.shape
    part = features // 4
    width = up.shape[1]
    out_width = down.shape[1]

    def f_cols(i):
        return pl.ds(pl.multiple_of(i * part, part), part)

    def half_cols(i):
        return pl.ds(pl.multiple_of((i % 2) * 2 * part, 2 * part), 2 * part)

    def h_cols(i):
        return pl.ds(pl.multiple_of(i * width, 128), width)

    def piece(slot, c):
        size = capacity // PARTS[slot]
        return pl.ds(c * size, size)

    barrier = pltpu.get_barrier_semaphore()
    for j in range(1, n):
        pl.semaphore_signal(barrier, inc=1, device_id={"ep": (e + j) % n}, device_id_type=MESH)
    for other in (mate, across):
        pl.semaphore_signal(barrier, inc=1, device_id={"tp": other}, device_id_type=MESH)
    rows_step = tokens // 4

    def token_load(i):
        rows = pl.ds(pl.multiple_of(i * rows_step, rows_step), rows_step)
        return pltpu.make_async_copy(tok_hbm.at[rows], tok_ref.at[rows], load_sems.at[i])

    sources = (
        (gain_hbm, gain_ref),
        (route_hbm, route_ref),
        (up_hbm.at[0], up),
        (scan_hbm, scan_ref),
        (taps_hbm, taps_ref),
        (lane_hbm, lane_ref),
        (jump_hbm, jump_ref),
        (carry_w_hbm, carry_w_ref),
        (entry_w_hbm, entry_w_ref),
        (score_hbm, score_ref),
        (valve_hbm, valve_ref),
        (down_hbm.at[0], down),
    )
    loads = [
        pltpu.make_async_copy(origin, place, load_sems.at[4 + i])
        for i, (origin, place) in enumerate(sources)
    ]
    for i in range(4):
        token_load(i).start()
    for load in loads:
        load.start()
    load_gain, load_route, load_up = loads[:3]
    load_scan, load_late, load_down = loads[3], loads[4:11], loads[11]
    channels, length = scan_ref.shape

    def norm_rows(i, _):
        rows = pl.ds(pl.multiple_of(i * rows_step, rows_step), rows_step)
        token_load(i).wait()
        x = tok_ref[rows, :].astype(jnp.float32)
        centered = x - jnp.sum(x, axis=1, keepdims=True) * (1.0 / features)
        var = jnp.sum(centered * centered, axis=1, keepdims=True) * (1.0 / features)
        normed[rows, :] = (centered * lax.rsqrt(var + 1e-05) * gain_ref[...]).astype(jnp.bfloat16)
        return 0

    with jax.named_scope("rank"):
        load_route.wait()
        routes = route_ref[...].astype(jnp.float32)
        first, second = routes[0:1, :], routes[1:2, :]
        erow = lax.broadcasted_iota(jnp.int32, (rank_rows.shape[0], tokens), 0).astype(jnp.float32)
        hit = (erow == first) | (erow == second)
        ti = lax.broadcasted_iota(jnp.int32, (tokens, tokens), 0)
        tj = lax.broadcasted_iota(jnp.int32, (tokens, tokens), 1)
        rank = jnp.dot(
            hit.astype(jnp.float32).astype(jnp.bfloat16),
            (ti < tj).astype(jnp.float32).astype(jnp.bfloat16),
            preferred_element_type=jnp.float32,
        )
        rank_rows[...] = jnp.where(hit, rank, -1.0)

    with jax.named_scope("norm"):
        load_gain.wait()
        lax.fori_loop(0, tokens // rows_step, norm_rows, 0)

    def picker(expert, start, size):
        slots = start + lax.broadcasted_iota(jnp.int32, (size, tokens), 0)
        hits = slots.astype(jnp.float32) == rank_rows[pl.ds(expert, 1), :]
        return hits.astype(jnp.float32).astype(jnp.bfloat16)

    with jax.named_scope("barrier"):
        pl.semaphore_wait(barrier, n + 1)

    send_halo = remote(halo_out, halo, halo_sems, 0, ep=(e + 1) % n)
    sent = [send_halo]
    waited = []

    def begin(copy):
        copy.start()

    def token_copy(role, c):
        rows = piece(role, c)
        if role == NEAR:
            origin, cols = near_rows.at[rows], half_cols(t)
        else:
            origin, cols = cross_rows.at[role - INNER, rows], f_cols(t)
        slot = slot_there[role]
        return pltpu.make_async_remote_copy(
            src_ref=origin,
            dst_ref=toks.at[slot, rows, cols],
            send_sem=out_sems.at[0],
            recv_sem=zt.at[slot - 1, c],
            device_id={"ep": peer[role]},
            device_id_type=MESH,
        )

    def token_arrival(slot, c):
        rows = piece(slot, c)
        cols = half_cols(t) if slot == NEAR else f_cols(t)
        view = toks.at[slot, rows, cols]
        return pltpu.make_async_remote_copy(
            src_ref=view,
            dst_ref=view,
            send_sem=out_sems.at[0],
            recv_sem=zt.at[slot - 1, c],
            device_id={"ep": peer[slot]},
            device_id_type=MESH,
        )

    def shared(view, sems, slot, c, target):
        kind, first, sems = sems
        return pltpu.make_async_remote_copy(
            src_ref=view,
            dst_ref=view,
            send_sem=out_sems.at[kind],
            recv_sem=sems.at[slot - first, c],
            device_id={"tp": target},
            device_id_type=MESH,
        )

    def tok_view(slot, c, owner):
        cols = half_cols(owner) if slot == NEAR else f_cols(owner)
        return toks.at[slot, piece(slot, c), cols]

    def hid_view(slot, c, owner):
        return hid.at[slot, piece(slot, c), h_cols(owner)]

    def result_copy(slot, c):
        rows = piece(slot, c)
        there = slot_there[slot]
        return pltpu.make_async_remote_copy(
            src_ref=res.at[slot, rows],
            dst_ref=back.at[there, rows],
            send_sem=out_sems.at[1],
            recv_sem=rz.at[there - 1, c],
            device_id={"ep": peer[slot]},
            device_id_type=MESH,
        )

    def result_arrival(role, c):
        view = back.at[role, piece(role, c)]
        return pltpu.make_async_remote_copy(
            src_ref=view,
            dst_ref=view,
            send_sem=out_sems.at[1],
            recv_sem=rz.at[role - 1, c],
            device_id={"ep": peer[role]},
            device_id_type=MESH,
        )

    def dispatch(role, c):
        size = capacity // PARTS[role]
        pick = picker(peer[role], c * size, size)
        if role == NEAR:
            picked = jnp.dot(pick, normed[:, half_cols(t)], preferred_element_type=jnp.float32)
            near_rows[piece(role, c), :] = picked.astype(jnp.bfloat16)
        else:
            picked = jnp.dot(pick, normed[:, f_cols(t)], preferred_element_type=jnp.float32)
            cross_rows[role - INNER, piece(role, c), :] = picked.astype(jnp.bfloat16)
        begin(token_copy(role, c))

    def first_matmul(slot, c):
        rows = piece(slot, c)
        for start in range(0, width, 256):
            size = min(256, width - start)
            value = jnp.dot(
                toks[slot, rows, :],
                up[:, start : start + size],
                preferred_element_type=jnp.float32,
            )
            value = value * jax.nn.sigmoid(value)
            cols = pl.ds(pl.multiple_of(t * width + start, 128), size)
            hid[slot, rows, cols] = value.astype(jnp.bfloat16)
        begin(shared(hid_view(slot, c, t), hx, slot, c, across))
        begin(shared(hid_view(slot, c, t), hm, slot, c, mate))

    def own_tokens(_, c):
        size = capacity // PARTS[OWN]
        mine = picker(e, c * size, size)
        for q in range(4):
            cols = slice(q * part, (q + 1) * part)
            picked = jnp.dot(mine, normed[:, cols], preferred_element_type=jnp.float32)
            toks[OWN, piece(OWN, c), cols] = picked.astype(jnp.bfloat16)
        if "up" not in waited:
            load_up.wait()
            waited.append("up")
        first_matmul(OWN, c)

    def spread(slot, c):
        token_arrival(slot, c).wait_recv()
        begin(shared(tok_view(slot, c, t), tm, slot, c, mate))
        if slot != NEAR:
            begin(shared(tok_view(slot, c, t), tx, slot, c, across))

    def forward(slot, c):
        if slot != NEAR:
            shared(tok_view(slot, c, across), tx, slot, c, across).wait_recv()
            begin(shared(tok_view(slot, c, across), tf, slot, c, mate))

    def hidden_block(slot, c):
        shared(tok_view(slot, c, mate), tm, slot, c, mate).wait_recv()
        if slot != NEAR:
            shared(tok_view(slot, c, far), tf, slot, c, mate).wait_recv()
        first_matmul(slot, c)

    def k_dot(slot, rows, first_row, size):
        cols = pl.ds(pl.multiple_of(first_row, 128), size)
        return jnp.dot(hid[slot, rows, cols], down[cols, :], preferred_element_type=jnp.float32)

    def gather_block(slot, c):
        rows = piece(slot, c)
        shared(hid_view(slot, c, across), hx, slot, c, across).wait_recv()
        begin(shared(hid_view(slot, c, across), hf, slot, c, mate))
        shared(hid_view(slot, c, mate), hm, slot, c, mate).wait_recv()
        if "down" not in waited:
            load_down.wait()
            waited.append("down")
        local = k_dot(slot, rows, (t // 2) * 2 * width, 2 * width)
        acc[slot, rows, :] = local + k_dot(slot, rows, across * width, width)

    def finish_block(slot, c):
        rows = piece(slot, c)
        shared(hid_view(slot, c, far), hf, slot, c, mate).wait_recv()
        res[slot, rows, :] = (acc[slot, rows, :] + k_dot(slot, rows, far * width, width)).astype(
            jnp.bfloat16
        )
        if slot != OWN:
            begin(result_copy(slot, c))

    blocks, size_w = carry_w_ref.shape[0], carry_w_ref.shape[1]

    def gate(w_ref, conv_half):
        whole = jnp.zeros((channels, channels), jnp.float32)
        for b in range(blocks):
            tall = (
                lax.broadcasted_iota(jnp.int32, (channels, size_w), 0)
                == lax.broadcasted_iota(jnp.int32, (channels, size_w), 1) + b * size_w
            )
            wide = (
                lax.broadcasted_iota(jnp.int32, (size_w, channels), 1)
                == lax.broadcasted_iota(jnp.int32, (size_w, channels), 0) + b * size_w
            )
            right = jnp.dot(
                w_ref[b],
                wide.astype(jnp.float32).astype(jnp.bfloat16),
                preferred_element_type=jnp.float32,
            ).astype(jnp.bfloat16)
            whole = whole + jnp.dot(
                tall.astype(jnp.float32).astype(jnp.bfloat16),
                right,
                preferred_element_type=jnp.float32,
            )
        return jax.nn.sigmoid(
            jnp.dot(conv_half, whole.astype(jnp.bfloat16), preferred_element_type=jnp.float32)
        )

    def carry_copy(j):
        return remote(carry_out, carry_in.at[j], carry_sems, j, ep=(e + n - j) % n)

    def halo_out_now():
        load_scan.wait()
        turned = scan_ref[...].astype(jnp.float32).T
        padded[HALO:, :] = turned
        halo_out[...] = turned[length - HALO :, :].astype(jnp.bfloat16)
        send_halo.start()

    def scan_local():
        for load in load_late:
            load.wait()
        send_halo.wait_recv()
        padded[0:HALO, :] = jnp.where(e > 0, halo[...].astype(jnp.float32), 0.0)
        taps = taps_ref[...].astype(jnp.float32)
        conv = jnp.zeros((length, channels), jnp.float32)
        for k in range(CONV):
            lead = HALO - (CONV - 1) + k
            conv = conv + padded[lead : lead + length, :] * taps[k : k + 1, :]
        conv_half = conv.astype(jnp.bfloat16)
        conv_buf[...] = conv
        lane = -lane_ref[...].reshape(1, channels)
        soft = jnp.maximum(lane, 0.0) + jnp.log1p(jnp.exp(-jnp.abs(lane)))
        fade = -8.0 * gate(carry_w_ref, conv_half) * soft + as_column(jump_ref[...])
        state = jnp.sqrt(one_minus_exp(2.0 * fade)) * gate(entry_w_ref, conv_half) * conv_buf[...]
        decay = jnp.exp(fade)
        place = lax.broadcasted_iota(jnp.int32, (length, channels), 0)
        shift = 1
        while shift < length:
            older_decay = jnp.where(place < shift, 1.0, pltpu.roll(decay, shift, 0))
            older_state = jnp.where(place < shift, 0.0, pltpu.roll(state, shift, 0))
            state = decay * older_state + state
            decay = decay * older_decay
            shift *= 2
        decay_buf[...] = decay
        state_buf[...] = state
        carry_out[0:8, :] = jnp.broadcast_to(decay[length - 1 : length, :], (8, channels))
        carry_out[8:16, :] = jnp.broadcast_to(state[length - 1 : length, :], (8, channels))
        for j in range(1, n):
            begin(carry_copy(j))
            sent.append(carry_copy(j))

    def scan_finish():
        entering = jnp.zeros((1, channels), jnp.float32)
        for j in range(1, n):
            carry_copy(j).wait_recv()
        for origin in range(n - 1):
            slot = (origin + n - e) % n
            slot = jnp.where(slot == 0, 1, slot)
            early = carry_in[slot]
            after = early[0:1, :] * entering + early[8:9, :]
            entering = jnp.where(origin < e, after, entering)
        gelu_in = valve_ref[...].astype(jnp.float32)
        inner = 0.7978845608028654 * (gelu_in + 0.044715 * (gelu_in * gelu_in * gelu_in))
        gelu = gelu_in * (0.5 * (1.0 + jnp.tanh(inner)))
        final = (state_buf[...] + decay_buf[...] * entering).T
        scan_out[...] = (final * gelu).astype(jnp.bfloat16)

    def plan_combine():
        first_col, second_col = as_column(first), as_column(second)
        scores = score_ref[...]
        first_weight = jax.nn.sigmoid(as_column(scores[0:1, :] - scores[1:2, :]))
        slots = lax.broadcasted_iota(jnp.int32, (tokens, capacity), 1).astype(jnp.float32)
        for role in (OWN, NEAR, INNER, OUTER):
            expert = peer.get(role, e)
            number = expert.astype(jnp.float32)
            rank_col = as_column(rank_rows[pl.ds(expert, 1), :])
            chosen[role] = (slots == rank_col).astype(jnp.float32).astype(jnp.bfloat16)
            weight = jnp.where(first_col == number, first_weight, 0.0) + jnp.where(
                second_col == number, 1.0 - first_weight, 0.0
            )
            share[role] = jnp.broadcast_to(weight, (tokens, 128))

    added = []

    def combine(role):
        if role != OWN:
            for c in range(PARTS[role]):
                result_arrival(role, c).wait_recv()
        source = res[OWN] if role == OWN else back[role]
        term = jnp.dot(chosen[role], source, preferred_element_type=jnp.float32)
        term = term * jnp.tile(share[role], (1, out_width // 128))
        if added:
            term = total[...] + term
        added.append(role)
        if len(added) == n:
            moe_out[...] = term.astype(jnp.bfloat16)
        else:
            total[...] = term

    tasks = {
        "D": dispatch,
        "P": own_tokens,
        "T": spread,
        "F": forward,
        "M": hidden_block,
        "G": gather_block,
        "S": finish_block,
    }
    for name in ORDER:
        with jax.named_scope(name):
            if name == "A":
                scan_local()
            elif name == "H":
                halo_out_now()
            elif name == "B":
                scan_finish()
                plan_combine()
            elif name[0] == "C":
                combine(int(name[1]))
            else:
                tasks[name[0]](int(name[1]), int(name[2]) - 1)

    def sent_all(kind, view):
        pltpu.make_async_remote_copy(
            src_ref=view,
            dst_ref=view,
            send_sem=out_sems.at[kind],
            recv_sem=out_sems.at[kind],
            device_id={"tp": mate},
            device_id_type=MESH,
        ).wait_send()

    with jax.named_scope("drain"):
        sent_all(0, toks.at[:, :, f_cols(t)])
        sent_all(1, res.at[pl.ds(NEAR, n - 1)])
        sent_all(2, toks.at[pl.ds(INNER, 2), :, f_cols(t)])
        sent_all(3, toks.at[:, :, f_cols(t)])
        sent_all(4, toks.at[pl.ds(INNER, 2), :, f_cols(t)])
        for kind in (5, 6, 7):
            sent_all(kind, hid.at[:, :, h_cols(t)])
        for copy in sent:
            copy.wait_send()


def slots_per_expert(tokens, top_count, experts, tp_size):
    return tp_size * ((3 * tokens * top_count + 2 * experts * tp_size - 1) // (2 * experts * tp_size))


def write_out(turned_ref, moe_ref, turned_out, moe_out, sems):
    copies = (
        pltpu.make_async_copy(turned_ref, turned_out, sems.at[0]),
        pltpu.make_async_copy(moe_ref, moe_out, sems.at[1]),
    )
    for copy in copies:
        copy.start()
    for copy in copies:
        copy.wait()


def fused(*arrays):
    (scan, valve, taps, carry_w, entry_w, lane, jump, tok, gain, routes, scores, up, down) = arrays
    n = lax.axis_size("ep")
    length, channels = scan.shape
    tokens, features = tok.shape
    width, out_width = up.shape[2], down.shape[2]
    units = down.shape[1]
    capacity = slots_per_expert(tokens, routes.shape[1], n, lax.axis_size("tp"))
    half, full = jnp.bfloat16, jnp.float32
    vmem = pl.BlockSpec(memory_space=pltpu.VMEM)
    hbm = pl.BlockSpec(memory_space=pl.ANY)
    pair = pltpu.SemaphoreType.DMA((2, n))
    most = max(PARTS.values())
    two, three, four = (pltpu.SemaphoreType.DMA((k, most)) for k in (2, 3, 4))
    small = (
        scan.T,
        valve.T,
        taps,
        carry_w,
        entry_w,
        lane,
        jump.reshape(1, -1),
        tok,
        gain.reshape(1, -1),
        routes.T,
        scores.T,
    )
    turned, moe = pl.pallas_call(
        functools.partial(fused_kernel, n, capacity),
        out_shape=(
            pltpu.VMEM((channels, length), half),
            pltpu.VMEM((tokens, out_width), half),
        ),
        in_specs=[hbm] * 13,
        out_specs=(vmem, vmem),
        scratch_shapes=[
            *(pltpu.VMEM(a.shape, a.dtype) for a in small),
            pltpu.VMEM((features, width), half),
            pltpu.VMEM((units, out_width), half),
            pltpu.VMEM((tokens, features), half),
            pltpu.VMEM((-(-n // 8) * 8, tokens), full),
            pltpu.VMEM((capacity, features // 2), half),
            pltpu.VMEM((2, capacity, features // 4), half),
            pltpu.VMEM((n, capacity, features), half),
            pltpu.VMEM((n, capacity, units), half),
            pltpu.VMEM((n, capacity, out_width), half),
            pltpu.VMEM((n, capacity, out_width), half),
            pltpu.VMEM((n, capacity, out_width), full),
            pltpu.VMEM((n, tokens, capacity), half),
            pltpu.VMEM((n, tokens, 128), full),
            pltpu.VMEM((tokens, out_width), full),
            pltpu.VMEM((HALO, channels), half),
            pltpu.VMEM((length + HALO, channels), full),
            pltpu.VMEM((length, channels), full),
            pltpu.VMEM((length, channels), full),
            pltpu.VMEM((length, channels), full),
            pltpu.VMEM((16, channels), full),
            pltpu.VMEM((n, 16, channels), full),
            pltpu.VMEM((HALO, channels), half),
            pltpu.SemaphoreType.DMA((16,)),
            three,
            two,
            three,
            two,
            *([four] * 3),
            three,
            pltpu.SemaphoreType.DMA((8,)),
            pltpu.SemaphoreType.DMA((2, 1)),
            pair,
        ],
        compiler_params=pltpu.CompilerParams(
            collective_id=0, has_side_effects=True, vmem_limit_bytes=56 * 1024 * 1024
        ),
    )(*small, up, down)
    turned, moe = pl.pallas_call(
        write_out,
        out_shape=(
            jax.ShapeDtypeStruct((channels, length), half),
            jax.ShapeDtypeStruct((tokens, out_width), half),
        ),
        in_specs=[hbm] * 2,
        out_specs=(hbm, hbm),
        scratch_shapes=[pltpu.SemaphoreType.DMA((2,))],
        compiler_params=pltpu.CompilerParams(vmem_limit_bytes=2 * 1024 * 1024),
    )(turned, moe)
    return turned.T, moe


def fits_fused(tok, routes, up, down):
    n, tp_size = lax.axis_size("ep"), lax.axis_size("tp")
    if tp_size != 4 or n != 4 or up.shape[0] != 1 or routes.shape[1] != 2:
        return False
    capacity = slots_per_expert(tok.shape[0], 2, n, tp_size)
    if capacity % 96 or tok.shape[0] % 32 or up.shape[2] % 128 or down.shape[2] % 256:
        return False
    held = n * capacity * (tok.shape[1] + down.shape[1] + 4 * down.shape[2])
    return 2 * (held + up.size + down.size + 3 * tok.size) < 44 * 1024 * 1024


def on_device(
    scan_branch_source,
    valve_branch_source,
    stencil_factors,
    carry_valve_matrix,
    entry_valve_matrix,
    lane_fade_param,
    jump_log_fade,
    specialist_entries,
    specialist_rms_scale,
    assigned_specialists,
    picked_route_scores,
    expand_matrix,
    contract_matrix,
):
    if fits_fused(specialist_entries, assigned_specialists, expand_matrix, contract_matrix):
        return fused(
            scan_branch_source,
            valve_branch_source,
            stencil_factors,
            carry_valve_matrix,
            entry_valve_matrix,
            lane_fade_param,
            jump_log_fade,
            specialist_entries,
            specialist_rms_scale,
            assigned_specialists,
            picked_route_scores,
            expand_matrix,
            contract_matrix,
        )
    valved_scan_target = temporal_block_part(
        scan_branch_source,
        valve_branch_source,
        stencil_factors,
        carry_valve_matrix,
        entry_valve_matrix,
        lane_fade_param,
        jump_log_fade,
    )
    moe_out = expert_part(
        specialist_entries,
        specialist_rms_scale,
        assigned_specialists,
        picked_route_scores,
        expand_matrix,
        contract_matrix,
    )
    return (valved_scan_target, moe_out)


def solution(mesh):
    placed = (
        P(("grp", "ep"), "tp"),
        P(("grp", "ep"), "tp"),
        P(None, "tp"),
        P("tp", None, None),
        P("tp", None, None),
        P("tp"),
        P(("grp", "ep")),
        P(("grp", "ep"), None),
        P(),
        P(("grp", "ep"), None),
        P(("grp", "ep"), None),
        P("ep", None, "tp"),
        P("ep", None, "tp"),
    )
    return jax.shard_map(
        on_device,
        mesh=mesh,
        in_specs=placed,
        out_specs=(P(("grp", "ep"), "tp"), P(("grp", "ep"), "tp")),
        check_vma=False,
    )
```
